512 devices in a mesh: row: 32 (over z, x), col: 16 (over y, core).
Axes of the slice: x: 4, y: 8, z: 8, core: 2. Of those that a mesh axis runs over, the one named last changes fastest.
Arguments:
- tokens: bfloat16 [32768, 2048], P('row'), may hold values from -136 to 136
- norm_gain: float32 [2048], replicated, may hold values from 0.1 to 1.9
- w_in: bfloat16 [2048, 1024], P(None, 'col'), may hold values from -0.125 to 0.125
- w_out: bfloat16 [1024, 2048], P(None, 'col'), may hold values from -0.1875 to 0.1875
Outputs:
- mixed_tokens: bfloat16 [32768, 2048], P('row', 'col')
The draws below stay inside these ranges and needn't reach their ends.
All inputs are finite; a program needn't handle non-finite values.
Results may differ from the reference program's by a relative error of at most 0.013.
Values may be sent and summed in bfloat16 or wider, within the bound.
No kernel may reach another device: no remote copies, remote signals or barrier semaphores. Data moves between devices by JAX's collectives and lax.ppermute only.
A program may use at most 64 MiB of HBM per device.

```python
import math
import jax
import jax.numpy as jnp
from jax import lax

D = 2048
FW = 1024
GROUP = 256
GROUPS = 4
LENGTH = 32768


def draw_tokens(key, part):
    key_values, key_scales = jax.random.split(key, 2)
    columns = jnp.arange(D, dtype=jnp.float32) / D
    values = jnp.clip(jax.random.normal(key_values, (LENGTH, D), jnp.float32), -6.0, 6.0)
    row_scale = jnp.exp(jax.random.uniform(key_scales, (LENGTH, 1), jnp.float32, 0.0, 0.2))
    col_scale = jnp.exp(columns * math.log(4.0))
    return (values * row_scale * col_scale[None, :]).astype(jnp.bfloat16)


def level_of(own_key, extent, cuts, smallest, high):
    factor_of, own = 1.0, jax.random.fold_in(own_key, 6)
    for position, shards_of in cuts:
        steps = jnp.exp(jax.random.uniform(jax.random.fold_in(own, position), (shards_of,), jnp.float32, smallest / len(cuts), high / len(cuts)))
        factor_of = factor_of * jnp.repeat(steps, extent[position] // shards_of).reshape([-1 if axis == position else 1 for axis in range(len(extent))])
    return factor_of


def bell_draw(rng, dims, spread, most, cuts=(), kind=jnp.bfloat16):
    drawn = jax.random.normal(rng, dims, jnp.float32) * spread
    if len(cuts) > 0:
        drawn = level_of(rng, dims, cuts, -0.22, 0.18) * drawn
    return jnp.clip(drawn, min=-most, max=most).astype(kind)


def setup_inputs(seed: int = 0) -> dict:
    keys = jax.random.split(jax.random.key(seed), 5)
    tokens = draw_tokens(jax.random.fold_in(keys[4], 71), 0)
    norm_gain = jnp.clip(1.0 + 0.18 * jax.random.normal(keys[1], (D,), jnp.float32), 0.1, 1.9)
    w_in = bell_draw(keys[2], (D, FW), D ** -0.5, 0.125, ((1, 16),))
    w_out = bell_draw(keys[3], (FW, D), FW ** -0.5, 0.1875, ((1, 16),))
    return {"tokens": tokens, "norm_gain": norm_gain, "w_in": w_in, "w_out": w_out}


NORM_EPS = 1e-06

def reference(tokens, norm_gain, w_in, w_out):
    widened = tokens.astype(jnp.float32)
    inverse = lax.rsqrt(lax.optimization_barrier(jnp.mean(widened * widened, axis=1, keepdims=True)) + NORM_EPS)
    normed = (widened * inverse * norm_gain[None, :]).astype(jnp.bfloat16)
    projected = jnp.dot(normed, w_in, preferred_element_type=jnp.float32).astype(jnp.bfloat16)
    grouped = projected.astype(jnp.float32).reshape(LENGTH, GROUPS, GROUP)
    spectrum = jnp.real(jnp.fft.fftn(grouped, axes=(0, 2), norm='ortho'))
    spectral = spectrum.reshape(LENGTH, FW).astype(jnp.bfloat16)
    return jnp.dot(spectral, w_out, preferred_element_type=jnp.float32).astype(jnp.bfloat16)
```

```python
import math

import jax
import jax.numpy as jnp
import numpy as np
from jax import lax
from jax.experimental import pallas as pl
from jax.experimental.pallas import tpu as pltpu
from jax.sharding import Mesh
from jax.sharding import PartitionSpec as P

GROUP = 256
NORM_EPS = 1e-06
BLOCK = 128


def project_body(x_ref, w_ref, out_ref, scr):
    step = pl.program_id(0)
    x = x_ref[...]
    wide = x.astype(jnp.float32)
    inverse = lax.rsqrt(jnp.mean(wide * wide, axis=1, keepdims=True) + NORM_EPS)
    part = jnp.dot(x, w_ref[...], preferred_element_type=jnp.float32) * inverse
    turned = part.T
    half = turned.shape[0] // 2
    steps = pl.num_programs(0)
    scr[:, pl.ds(step, 1), :] = turned[:half].reshape(half, 1, BLOCK)
    scr[:, pl.ds(step + steps, 1), :] = turned[half:].reshape(half, 1, BLOCK)

    @pl.when(step == steps - 1)
    def _():
        out_ref[...] = scr[...].astype(jnp.bfloat16)


def project(tokens, weight):
    rows, width = tokens.shape
    channels = weight.shape[1]
    steps = rows // BLOCK
    shape = (channels // 2, 2 * steps, BLOCK)
    return pl.pallas_call(
        project_body,
        grid=(steps,),
        in_specs=[
            pl.BlockSpec((BLOCK, width), lambda s: (s, 0)),
            pl.BlockSpec((width, channels), lambda s: (0, 0)),
        ],
        out_specs=pl.BlockSpec(shape, lambda s: (0, 0, 0)),
        out_shape=jax.ShapeDtypeStruct(shape, jnp.bfloat16),
        scratch_shapes=[pltpu.VMEM(shape, jnp.float32)],
        compiler_params=pltpu.CompilerParams(dimension_semantics=("arbitrary",)),
    )(tokens, weight)


def fft_tables(total, n_first, n_second):
    scale = 1.0 / math.sqrt(total * GROUP)
    one = np.arange(n_first)
    two = np.arange(n_second)
    first = 2.0 * np.pi * (np.outer(one, one) % n_first) / n_first
    table_one = np.concatenate([np.cos(first), np.sin(first)], 0)
    turn = 2.0 * np.pi * np.outer(one, two) / total
    turns = np.stack([np.cos(turn), np.sin(turn)]) * scale
    second = 2.0 * np.pi * (np.outer(two, two) % n_second) / n_second
    cosine, sine = np.cos(second), np.sin(second)
    table_two = np.block([[cosine, sine], [-sine, cosine]])
    return (
        jnp.asarray(table_one, jnp.bfloat16),
        jnp.asarray(turns, jnp.float32),
        jnp.asarray(table_two, jnp.bfloat16),
    )


def positions_body(x_ref, one_ref, turn_ref, two_ref, out_ref, scr):
    wide = x_ref[...].astype(jnp.float32)
    n_first = wide.shape[0] * 8
    both = [
        wide[:, 8 * c : 8 * c + 8, :].reshape(n_first, BLOCK).astype(jnp.bfloat16)
        for c in range(2)
    ]
    cosine, sine = turn_ref[0], turn_ref[1]
    for c in range(2):
        y = jnp.dot(one_ref[...], both[c], preferred_element_type=jnp.float32)
        y_cos, y_sin = y[:n_first], y[n_first:]
        turned = jnp.concatenate(
            [y_cos * cosine - y_sin * sine, -(y_sin * cosine) - y_cos * sine], 1
        ).astype(jnp.bfloat16)
        z = lax.dot_general(
            two_ref[...], turned, (((1,), (1,)), ((), ())), preferred_element_type=jnp.float32
        )
        for part in range(2):
            for high in range(2):
                scr[:, 4 * c + 2 * part + high, :] = z[
                    BLOCK * part : BLOCK * part + BLOCK, BLOCK * high : BLOCK * high + BLOCK
                ]
    out_ref[...] = scr[...].astype(jnp.bfloat16)


def positions(arrived, total):
    rows = arrived.shape[0]
    tables = fft_tables(total, rows * 8, BLOCK)
    shape = (BLOCK, 8, BLOCK)
    return pl.pallas_call(
        positions_body,
        out_shape=jax.ShapeDtypeStruct(shape, jnp.bfloat16),
        scratch_shapes=[pltpu.VMEM(shape, jnp.float32)],
    )(arrived, *tables)


def channel_table(rows, near):
    source = np.arange(rows * near)
    channel = np.stack(
        [(GROUP // near) * (source % near) + source // near + rows * c for c in range(2)]
    )
    freq = np.arange(GROUP)
    phase = 2.0 * np.pi * (freq[:, None, None] * channel[None] % GROUP) / GROUP
    both = np.stack([np.cos(phase), np.sin(phase)], 2)
    return jnp.asarray(both.reshape(GROUP, -1), jnp.bfloat16)


def channels_body(x_ref, table_ref, out_ref, scr):
    scr[...] = x_ref[...].astype(jnp.float32)
    rows = [
        jnp.concatenate([scr[:, 2 * j, :], scr[:, 2 * j + 1, :]], 1).astype(jnp.bfloat16)
        for j in range(4)
    ]
    data = jnp.concatenate(rows, 0)
    spectrum = jnp.dot(table_ref[...], data, preferred_element_type=jnp.float32)
    out_ref[...] = spectrum.T.astype(jnp.bfloat16)


def channel_mix(arrived, table):
    count = arrived.shape[1] * arrived.shape[2] // 4
    return pl.pallas_call(
        channels_body,
        out_shape=jax.ShapeDtypeStruct((count, GROUP), jnp.bfloat16),
        scratch_shapes=[pltpu.VMEM(arrived.shape, jnp.float32)],
    )(arrived, table)


def output_body(half_ref, spec_ref, own_ref, other_ref, out_ref):
    half = half_ref[0]
    groups = spec_ref.shape[0]
    for k in range(2):
        for ref, place in ((own_ref, 2 * half + k), (other_ref, 2 * (1 - half) + k)):
            total = None
            for g in range(groups):
                part = jnp.dot(
                    spec_ref[g],
                    ref[k, GROUP * g : GROUP * g + GROUP, :],
                    preferred_element_type=jnp.float32,
                )
                total = part if total is None else total + part
            out_ref[pl.ds(place, 1)] = total.astype(jnp.bfloat16)[None]


def output_map(half, gathered, own, other):
    count = gathered.shape[1]
    return pl.pallas_call(
        output_body,
        in_specs=[
            pl.BlockSpec(memory_space=pltpu.SMEM),
            pl.BlockSpec(memory_space=pltpu.VMEM),
            pl.BlockSpec(memory_space=pltpu.VMEM),
            pl.BlockSpec(memory_space=pltpu.VMEM),
        ],
        out_shape=jax.ShapeDtypeStruct((4, count, own.shape[2]), jnp.bfloat16),
    )(half, gathered, own, other)


def local(tokens, norm_gain, w_in, w_out):
    rows = lax.axis_size("row")
    total = tokens.shape[0] * rows
    own = lax.all_gather(w_out, "k", axis=0)
    other = lax.ppermute(own, "h", [(0, 1), (1, 0)])
    weight = (w_in.astype(jnp.float32) * norm_gain[:, None]).astype(jnp.bfloat16)
    projected = project(tokens, weight)
    arrived = lax.all_to_all(projected, "row", 0, 0, tiled=True)
    spectra = positions(arrived, total)
    arrived = lax.all_to_all(spectra, ("row", "h", "k"), 0, 0, tiled=True)
    mixed = channel_mix(arrived, channel_table(rows, 4))
    gathered = lax.all_gather(mixed, "g", axis=0)
    half = lax.axis_index("h").astype(jnp.int32).reshape(1)
    output = output_map(half, gathered, own, other)
    output = lax.all_to_all(output, ("h", "k"), 0, 0, tiled=True)
    return output.reshape(tokens.shape[0], w_out.shape[1])


def solution(mesh):
    mesh = Mesh(mesh.devices.reshape(32, 4, 2, 2), ("row", "g", "h", "k"))
    columns = ("g", "h", "k")
    placed = (P("row", None), P(), P(None, columns), P(None, columns))
    return jax.shard_map(
        local, mesh=mesh, in_specs=placed, out_specs=P("row", columns), check_vma=False
    )
```

```python
import math

import jax
import jax.numpy as jnp
import numpy as np
from jax import lax
from jax.experimental import pallas as pl
from jax.experimental.pallas import tpu as pltpu
from jax.sharding import Mesh
from jax.sharding import PartitionSpec as P

GROUP = 256
NORM_EPS = 1e-06
BLOCK = 128
SMALL = pltpu.CompilerParams(vmem_limit_bytes=16 << 20)


def project_body(x_hbm, w_hbm, gain_hbm, out_ref, x_buf, w_buf, gain_buf, scr, sems):
    pieces = sems.shape[0] - 2
    rows = x_buf.shape[0] // pieces
    weights = pltpu.make_async_copy(w_hbm, w_buf, sems.at[pieces])
    gains = pltpu.make_async_copy(gain_hbm, gain_buf, sems.at[pieces + 1])
    weights.start()
    gains.start()
    copies = []
    for j in range(pieces):
        span = pl.ds(rows * j, rows)
        copies.append(pltpu.make_async_copy(x_hbm.at[span], x_buf.at[span], sems.at[j]))
        copies[j].start()
    weights.wait()
    gains.wait()
    weight = (w_buf[...].astype(jnp.float32) * gain_buf[...]).T.astype(jnp.bfloat16)
    half = weight.shape[1] // 2
    blocks = x_buf.shape[0] // BLOCK
    for j in range(pieces):
        copies[j].wait()
        x = x_buf[rows * j : rows * j + rows, :]
        wide = x.astype(jnp.float32)
        inverse = lax.rsqrt(jnp.mean(wide * wide, axis=1, keepdims=True) + NORM_EPS)
        turned = (jnp.dot(x, weight, preferred_element_type=jnp.float32) * inverse).T
        for b in range(rows // BLOCK):
            for c in range(2):
                place = rows // BLOCK * j + b + blocks * c
                scr[:, place, :] = turned[half * c : half * c + half, BLOCK * b : BLOCK * b + BLOCK]
    out_ref[...] = scr[...].astype(jnp.bfloat16)


def project(tokens, w_in, gain):
    rows, width = tokens.shape
    channels = w_in.shape[1]
    pieces = 4
    shape = (channels // 2, 2 * rows // BLOCK, BLOCK)
    inputs = [
        pltpu.with_memory_space_constraint(a, pltpu.HBM) for a in (tokens, w_in.T, gain[None])
    ]
    return pl.pallas_call(
        project_body,
        in_specs=[pl.BlockSpec(memory_space=pltpu.HBM)] * 3,
        out_specs=pl.BlockSpec(memory_space=pltpu.VMEM),
        out_shape=pltpu.VMEM(shape, jnp.bfloat16),
        scratch_shapes=[
            pltpu.VMEM((rows, width), jnp.bfloat16),
            pltpu.VMEM((channels, width), jnp.bfloat16),
            pltpu.VMEM((1, width), jnp.float32),
            pltpu.VMEM(shape, jnp.float32),
            pltpu.SemaphoreType.DMA((pieces + 2,)),
        ],
        compiler_params=pltpu.CompilerParams(vmem_limit_bytes=24 << 20),
    )(*inputs)


def fft_tables(total, n_first, n_second):
    scale = 1.0 / math.sqrt(total * GROUP)
    one = np.arange(n_first)
    two = np.arange(n_second)
    first = 2.0 * np.pi * (np.outer(one, one) % n_first) / n_first
    table_one = np.concatenate([np.cos(first), np.sin(first)], 0)
    turn = 2.0 * np.pi * np.outer(one, two) / total
    turns = np.stack([np.cos(turn), np.sin(turn)]) * scale
    second = 2.0 * np.pi * (np.outer(two, two) % n_second) / n_second
    cosine, sine = np.cos(second), np.sin(second)
    table_two = np.block([[cosine, sine], [-sine, cosine]])
    return (
        jnp.asarray(table_one, jnp.bfloat16),
        jnp.asarray(turns, jnp.float32),
        jnp.asarray(table_two, jnp.bfloat16),
    )


def positions_body(x_ref, one_ref, turn_ref, two_ref, out_ref, scr):
    wide = x_ref[...].astype(jnp.float32)
    n_first = wide.shape[0] * 8
    both = [
        wide[:, 8 * c : 8 * c + 8, :].reshape(n_first, BLOCK).astype(jnp.bfloat16)
        for c in range(2)
    ]
    cosine, sine = turn_ref[0], turn_ref[1]
    for c in range(2):
        y = jnp.dot(one_ref[...], both[c], preferred_element_type=jnp.float32)
        y_cos, y_sin = y[:n_first], y[n_first:]
        turned = jnp.concatenate(
            [y_cos * cosine - y_sin * sine, -(y_sin * cosine) - y_cos * sine], 1
        ).astype(jnp.bfloat16)
        z = lax.dot_general(
            two_ref[...], turned, (((1,), (1,)), ((), ())), preferred_element_type=jnp.float32
        )
        for part in range(2):
            for high in range(2):
                scr[:, 4 * c + 2 * part + high, :] = z[
                    BLOCK * part : BLOCK * part + BLOCK, BLOCK * high : BLOCK * high + BLOCK
                ]
    out_ref[...] = scr[...].astype(jnp.bfloat16)


def positions(arrived, total):
    rows = arrived.shape[0]
    tables = fft_tables(total, rows * 8, BLOCK)
    shape = (BLOCK, 8, BLOCK)
    return pl.pallas_call(
        positions_body,
        out_shape=pltpu.VMEM(shape, jnp.bfloat16),
        scratch_shapes=[pltpu.VMEM(shape, jnp.float32)],
        compiler_params=SMALL,
    )(arrived, *tables)


def channel_table(rows, near):
    source = np.arange(rows * near)
    channel = np.stack(
        [(GROUP // near) * (source % near) + source // near + rows * c for c in range(2)]
    )
    freq = np.arange(GROUP)
    phase = 2.0 * np.pi * (freq[:, None, None] * channel[None] % GROUP) / GROUP
    both = np.stack([np.cos(phase), np.sin(phase)], 2)
    return jnp.asarray(both.reshape(GROUP, -1), jnp.bfloat16)


def channels_body(x_ref, table_ref, out_ref, scr):
    scr[...] = x_ref[...].astype(jnp.float32)
    rows = [
        jnp.concatenate([scr[:, 2 * j, :], scr[:, 2 * j + 1, :]], 1).astype(jnp.bfloat16)
        for j in range(4)
    ]
    data = jnp.concatenate(rows, 0)
    spectrum = jnp.dot(table_ref[...], data, preferred_element_type=jnp.float32)
    out_ref[...] = spectrum.T.astype(jnp.bfloat16)


def channel_mix(arrived, table):
    count = arrived.shape[1] * arrived.shape[2] // 4
    return pl.pallas_call(
        channels_body,
        out_shape=pltpu.VMEM((count, GROUP), jnp.bfloat16),
        scratch_shapes=[pltpu.VMEM(arrived.shape, jnp.float32)],
        compiler_params=SMALL,
    )(arrived, table)


def output_body(half_ref, spec_ref, own_ref, other_ref, out_ref):
    half = half_ref[0]
    groups = spec_ref.shape[0]
    for k in range(2):
        for ref, place in ((own_ref, 2 * half + k), (other_ref, 2 * (1 - half) + k)):
            total = None
            for g in range(groups):
                part = jnp.dot(
                    spec_ref[g],
                    ref[k, GROUP * g : GROUP * g + GROUP, :],
                    preferred_element_type=jnp.float32,
                )
                total = part if total is None else total + part
            out_ref[pl.ds(place, 1)] = total.astype(jnp.bfloat16)[None]


def output_map(half, gathered, own, other):
    count = gathered.shape[1]
    return pl.pallas_call(
        output_body,
        in_specs=[
            pl.BlockSpec(memory_space=pltpu.SMEM),
            pl.BlockSpec(memory_space=pltpu.VMEM),
            pl.BlockSpec(memory_space=pltpu.VMEM),
            pl.BlockSpec(memory_space=pltpu.VMEM),
        ],
        out_shape=pltpu.VMEM((4, count, own.shape[2]), jnp.bfloat16),
        compiler_params=SMALL,
    )(half, gathered, own, other)


def local(tokens, norm_gain, w_in, w_out):
    rows = lax.axis_size("row")
    total = tokens.shape[0] * rows
    own = lax.all_gather(w_out, "k", axis=0)
    other = lax.ppermute(own, "h", [(0, 1), (1, 0)])
    projected = project(tokens, w_in, norm_gain)
    arrived = lax.all_to_all(projected, "row", 0, 0, tiled=True)
    spectra = positions(arrived, total)
    arrived = lax.all_to_all(spectra, ("row", "h", "k"), 0, 0, tiled=True)
    mixed = channel_mix(arrived, channel_table(rows, 4))
    gathered = lax.all_gather(mixed, "g", axis=0)
    half = lax.axis_index("h").astype(jnp.int32).reshape(1)
    output = output_map(half, gathered, own, other)
    output = lax.all_to_all(output, ("h", "k"), 0, 0, tiled=True)
    return output.reshape(tokens.shape[0], w_out.shape[1])


def solution(mesh):
    mesh = Mesh(mesh.devices.reshape(32, 4, 2, 2), ("row", "g", "h", "k"))
    columns = ("g", "h", "k")
    placed = (P("row", None), P(), P(None, columns), P(None, columns))
    return jax.shard_map(
        local, mesh=mesh, in_specs=placed, out_specs=P("row", columns), check_vma=False
    )
```

```python
import math

import jax
import jax.numpy as jnp
import numpy as np
from jax import lax
from jax.experimental import pallas as pl
from jax.experimental.pallas import tpu as pltpu
from jax.sharding import Mesh
from jax.sharding import PartitionSpec as P

GROUP = 256
NORM_EPS = 1e-06
BLOCK = 128
AHEAD = 3
SMALL = pltpu.CompilerParams(vmem_limit_bytes=16 << 20)


def project_body(x_hbm, w_hbm, gain_hbm, out_ref, x_buf, w_buf, gain_buf, scr, sems):
    pieces = sems.shape[0] - 2
    rows = x_buf.shape[0] // pieces
    weights = pltpu.make_async_copy(w_hbm, w_buf, sems.at[pieces])
    gains = pltpu.make_async_copy(gain_hbm, gain_buf, sems.at[pieces + 1])
    weights.start()
    gains.start()
    copies = []
    for j in range(pieces):
        span = pl.ds(rows * j, rows)
        copies.append(pltpu.make_async_copy(x_hbm.at[span], x_buf.at[span], sems.at[j]))
    for j in range(AHEAD):
        copies[j].start()
    weights.wait()
    gains.wait()
    weight = (w_buf[...].astype(jnp.float32) * gain_buf[...]).T.astype(jnp.bfloat16)
    half = weight.shape[1] // 2
    blocks = x_buf.shape[0] // BLOCK


    def finish(j, part, square):
        turned = (part * lax.rsqrt(square + NORM_EPS)).T
        for b in range(rows // BLOCK):
            for c in range(2):
                place = rows // BLOCK * j + b + blocks * c
                scr[:, place, :] = turned[half * c : half * c + half, BLOCK * b : BLOCK * b + BLOCK]

    waiting = None
    for j in range(pieces):
        copies[j].wait()
        if j + AHEAD < pieces:
            copies[j + AHEAD].start()
        x = x_buf[rows * j : rows * j + rows, :]
        wide = x.astype(jnp.float32)
        square = jnp.mean(wide * wide, axis=1, keepdims=True)
        part = jnp.dot(x, weight, preferred_element_type=jnp.float32)
        if waiting is not None:
            finish(*waiting)
        waiting = (j, part, square)
    finish(*waiting)
    out_ref[...] = scr[...].astype(jnp.bfloat16)


def project(tokens, w_in, gain):
    rows, width = tokens.shape
    channels = w_in.shape[1]
    pieces = 4
    shape = (channels // 2, 2 * rows // BLOCK, BLOCK)
    inputs = [
        pltpu.with_memory_space_constraint(a, pltpu.HBM) for a in (tokens, w_in.T, gain[None])
    ]
    return pl.pallas_call(
        project_body,
        in_specs=[pl.BlockSpec(memory_space=pltpu.HBM)] * 3,
        out_specs=pl.BlockSpec(memory_space=pltpu.VMEM),
        out_shape=pltpu.VMEM(shape, jnp.bfloat16),
        scratch_shapes=[
            pltpu.VMEM((rows, width), jnp.bfloat16),
            pltpu.VMEM((channels, width), jnp.bfloat16),
            pltpu.VMEM((1, width), jnp.float32),
            pltpu.VMEM(shape, jnp.float32),
            pltpu.SemaphoreType.DMA((pieces + 2,)),
        ],
        compiler_params=pltpu.CompilerParams(vmem_limit_bytes=24 << 20),
    )(*inputs)


def fft_tables(total, n_first, n_second):
    scale = 1.0 / math.sqrt(total * GROUP)
    one = np.arange(n_first)
    two = np.arange(n_second)
    first = 2.0 * np.pi * (np.outer(one, one) % n_first) / n_first
    table_one = np.concatenate([np.cos(first), np.sin(first)], 0)
    turn = 2.0 * np.pi * np.outer(one, two) / total
    turns = np.stack([np.cos(turn), np.sin(turn)]) * scale
    second = 2.0 * np.pi * (np.outer(two, two) % n_second) / n_second
    cosine, sine = np.cos(second), np.sin(second)
    table_two = np.block([[cosine, sine], [-sine, cosine]])
    return (
        jnp.asarray(table_one, jnp.bfloat16),
        jnp.asarray(turns, jnp.float32),
        jnp.asarray(table_two, jnp.bfloat16),
    )


def positions_body(x_ref, one_ref, turn_ref, two_ref, out_ref, scr):
    wide = x_ref[...].astype(jnp.float32)
    n_first = wide.shape[0] * 8
    both = [
        wide[:, 8 * c : 8 * c + 8, :].reshape(n_first, BLOCK).astype(jnp.bfloat16)
        for c in range(2)
    ]
    cosine, sine = turn_ref[0], turn_ref[1]
    for c in range(2):
        y = jnp.dot(one_ref[...], both[c], preferred_element_type=jnp.float32)
        y_cos, y_sin = y[:n_first], y[n_first:]
        turned = jnp.concatenate(
            [y_cos * cosine - y_sin * sine, -(y_sin * cosine) - y_cos * sine], 1
        ).astype(jnp.bfloat16)
        z = lax.dot_general(
            two_ref[...], turned, (((1,), (1,)), ((), ())), preferred_element_type=jnp.float32
        )
        for part in range(2):
            for high in range(2):
                scr[:, 4 * c + 2 * part + high, :] = z[
                    BLOCK * part : BLOCK * part + BLOCK, BLOCK * high : BLOCK * high + BLOCK
                ]
    out_ref[...] = scr[...].astype(jnp.bfloat16)


def positions(arrived, total):
    rows = arrived.shape[0]
    tables = fft_tables(total, rows * 8, BLOCK)
    shape = (BLOCK, 8, BLOCK)
    return pl.pallas_call(
        positions_body,
        out_shape=pltpu.VMEM(shape, jnp.bfloat16),
        scratch_shapes=[pltpu.VMEM(shape, jnp.float32)],
        compiler_params=SMALL,
    )(arrived, *tables)


def channel_table(rows, near):
    source = np.arange(rows * near)
    channel = np.stack(
        [(GROUP // near) * (source % near) + source // near + rows * c for c in range(2)]
    )
    freq = np.arange(GROUP)
    phase = 2.0 * np.pi * (freq[:, None, None] * channel[None] % GROUP) / GROUP
    both = np.stack([np.cos(phase), np.sin(phase)], 2)
    return jnp.asarray(both.reshape(GROUP, -1), jnp.bfloat16)


def channels_body(x_ref, table_ref, out_ref, scr):
    scr[...] = x_ref[...].astype(jnp.float32)
    rows = [
        jnp.concatenate([scr[:, 2 * j, :], scr[:, 2 * j + 1, :]], 1).astype(jnp.bfloat16)
        for j in range(4)
    ]
    data = jnp.concatenate(rows, 0)
    spectrum = jnp.dot(table_ref[...], data, preferred_element_type=jnp.float32)
    out_ref[...] = spectrum.T.astype(jnp.bfloat16)


def channel_mix(arrived, table):
    count = arrived.shape[1] * arrived.shape[2] // 4
    return pl.pallas_call(
        channels_body,
        out_shape=pltpu.VMEM((count, GROUP), jnp.bfloat16),
        scratch_shapes=[pltpu.VMEM(arrived.shape, jnp.float32)],
        compiler_params=SMALL,
    )(arrived, table)


def output_body(place_ref, spec_ref, own_ref, other_ref, out_ref):
    half, core = place_ref[0], place_ref[1]
    groups = spec_ref.shape[0]
    spans = [
        pl.ds(pl.multiple_of(GROUP * jnp.where(core == 0, g, (groups - g) % groups), GROUP), GROUP)
        for g in range(groups)
    ]
    for k in range(2):
        for ref, place in ((own_ref, 2 * half + k), (other_ref, 2 * (1 - half) + k)):
            total = None
            for g in range(groups):
                part = jnp.dot(
                    spec_ref[g], ref[k, spans[g], :], preferred_element_type=jnp.float32
                )
                total = part if total is None else total + part
            out_ref[pl.ds(place, 1)] = total.astype(jnp.bfloat16)[None]


def output_map(place, gathered, own, other):
    count = gathered.shape[1]
    return pl.pallas_call(
        output_body,
        in_specs=[
            pl.BlockSpec(memory_space=pltpu.SMEM),
            pl.BlockSpec(memory_space=pltpu.VMEM),
            pl.BlockSpec(memory_space=pltpu.VMEM),
            pl.BlockSpec(memory_space=pltpu.VMEM),
        ],
        out_shape=pltpu.VMEM((4, count, own.shape[2]), jnp.bfloat16),
        compiler_params=SMALL,
    )(place, gathered, own, other)


def local(tokens, norm_gain, w_in, w_out):
    rows = lax.axis_size("row")
    total = tokens.shape[0] * rows
    own = lax.all_gather(w_out, "k", axis=0)
    other = lax.ppermute(own, "h", [(0, 1), (1, 0)])
    projected = project(tokens, w_in, norm_gain)
    arrived = lax.all_to_all(projected, "row", 0, 0, tiled=True)
    spectra = positions(arrived, total)
    arrived = lax.all_to_all(spectra, ("row", "h", "k"), 0, 0, tiled=True)
    mixed = channel_mix(arrived, channel_table(rows, 4))
    far = [
        [4 * (g if k == 0 else -g % 4) + 2 * h + k for g in range(4)]
        for h in range(2)
        for k in range(2)
    ]
    gathered = lax.all_gather(mixed, ("g", "h", "k"), axis=0, axis_index_groups=far)
    place = jnp.stack([lax.axis_index("h"), lax.axis_index("k")]).astype(jnp.int32)
    output = output_map(place, gathered, own, other)
    output = lax.all_to_all(output, ("h", "k"), 0, 0, tiled=True)
    return output.reshape(tokens.shape[0], w_out.shape[1])


def solution(mesh):
    mesh = Mesh(mesh.devices.reshape(32, 4, 2, 2), ("row", "g", "h", "k"))
    columns = ("g", "h", "k")
    placed = (P("row", None), P(), P(None, columns), P(None, columns))
    return jax.shard_map(
        local, mesh=mesh, in_specs=placed, out_specs=P("row", columns), check_vma=False
    )
```

```python
import math

import jax
import jax.numpy as jnp
import numpy as np
from jax import lax
from jax.experimental import pallas as pl
from jax.experimental.pallas import tpu as pltpu
from jax.sharding import Mesh
from jax.sharding import PartitionSpec as P

GROUP = 256
NORM_EPS = 1e-06
BLOCK = 128
AHEAD = 3
SMALL = pltpu.CompilerParams(vmem_limit_bytes=16 << 20)


def project_body(x_hbm, w_hbm, gain_hbm, out_ref, x_buf, w_buf, gain_buf, scr, sems):
    pieces = sems.shape[0] - 2
    rows = x_buf.shape[0] // pieces
    weights = pltpu.make_async_copy(w_hbm, w_buf, sems.at[pieces])
    gains = pltpu.make_async_copy(gain_hbm, gain_buf, sems.at[pieces + 1])
    weights.start()
    gains.start()
    copies = []
    for j in range(pieces):
        span = pl.ds(rows * j, rows)
        copies.append(pltpu.make_async_copy(x_hbm.at[span], x_buf.at[span], sems.at[j]))
    for j in range(AHEAD):
        copies[j].start()
    weights.wait()
    gains.wait()
    weight = (w_buf[...].astype(jnp.float32) * gain_buf[...]).T.astype(jnp.bfloat16)
    half = weight.shape[1] // 2
    blocks = x_buf.shape[0] // BLOCK


    def finish(j, part, square):
        turned = (part * lax.rsqrt(square + NORM_EPS)).T
        for b in range(rows // BLOCK):
            for c in range(2):
                place = rows // BLOCK * j + b + blocks * c
                scr[:, place, :] = turned[half * c : half * c + half, BLOCK * b : BLOCK * b + BLOCK]

    waiting = None
    for j in range(pieces):
        copies[j].wait()
        if j + AHEAD < pieces:
            copies[j + AHEAD].start()
        x = x_buf[rows * j : rows * j + rows, :]
        wide = x.astype(jnp.float32)
        square = jnp.mean(wide * wide, axis=1, keepdims=True)
        part = jnp.dot(x, weight, preferred_element_type=jnp.float32)
        if waiting is not None:
            finish(*waiting)
        waiting = (j, part, square)
    finish(*waiting)
    out_ref[...] = scr[...].astype(jnp.bfloat16)


def project(tokens, w_in, gain):
    rows, width = tokens.shape
    channels = w_in.shape[1]
    pieces = 4
    shape = (channels // 2, 2 * rows // BLOCK, BLOCK)
    inputs = [
        pltpu.with_memory_space_constraint(a, pltpu.HBM) for a in (tokens, w_in.T, gain[None])
    ]
    return pl.pallas_call(
        project_body,
        in_specs=[pl.BlockSpec(memory_space=pltpu.HBM)] * 3,
        out_specs=pl.BlockSpec(memory_space=pltpu.VMEM),
        out_shape=pltpu.VMEM(shape, jnp.bfloat16),
        scratch_shapes=[
            pltpu.VMEM((rows, width), jnp.bfloat16),
            pltpu.VMEM((channels, width), jnp.bfloat16),
            pltpu.VMEM((1, width), jnp.float32),
            pltpu.VMEM(shape, jnp.float32),
            pltpu.SemaphoreType.DMA((pieces + 2,)),
        ],
        compiler_params=pltpu.CompilerParams(vmem_limit_bytes=24 << 20),
    )(*inputs)


def fft_tables(total, n_first, n_second):
    scale = 1.0 / math.sqrt(total * GROUP)
    one = np.arange(n_first)
    two = np.arange(n_second)
    first = 2.0 * np.pi * (np.outer(one, one) % n_first) / n_first
    table_one = np.concatenate([np.cos(first), np.sin(first)], 0)
    turn = 2.0 * np.pi * np.outer(one, two) / total
    turns = np.stack([np.cos(turn), np.sin(turn)]) * scale
    second = 2.0 * np.pi * (np.outer(two, two) % n_second) / n_second
    cosine, sine = np.cos(second), np.sin(second)
    table_two = np.block([[cosine, sine], [-sine, cosine]])
    return (
        jnp.asarray(table_one, jnp.bfloat16),
        jnp.asarray(turns, jnp.float32),
        jnp.asarray(table_two, jnp.bfloat16),
    )


def positions_body(x_ref, one_ref, turn_ref, two_ref, out_ref, scr):
    wide = x_ref[...].astype(jnp.float32)
    n_first = wide.shape[0] * 8
    both = [
        wide[:, 8 * c : 8 * c + 8, :].reshape(n_first, BLOCK).astype(jnp.bfloat16)
        for c in range(2)
    ]
    cosine, sine = turn_ref[0], turn_ref[1]
    for c in range(2):
        y = jnp.dot(one_ref[...], both[c], preferred_element_type=jnp.float32)
        y_cos, y_sin = y[:n_first], y[n_first:]
        turned = jnp.concatenate(
            [y_cos * cosine - y_sin * sine, -(y_sin * cosine) - y_cos * sine], 1
        ).astype(jnp.bfloat16)
        z = lax.dot_general(
            two_ref[...], turned, (((1,), (1,)), ((), ())), preferred_element_type=jnp.float32
        )
        for part in range(2):
            for high in range(2):
                scr[:, 4 * c + 2 * part + high, :] = z[
                    BLOCK * part : BLOCK * part + BLOCK, BLOCK * high : BLOCK * high + BLOCK
                ]
    out_ref[...] = scr[...].astype(jnp.bfloat16)


def positions(arrived, total):
    rows = arrived.shape[0]
    tables = fft_tables(total, rows * 8, BLOCK)
    shape = (BLOCK, 8, BLOCK)
    return pl.pallas_call(
        positions_body,
        out_shape=pltpu.VMEM(shape, jnp.bfloat16),
        scratch_shapes=[pltpu.VMEM(shape, jnp.float32)],
        compiler_params=SMALL,
    )(arrived, *tables)


def channel_table(rows, near):
    source = np.arange(rows * near)
    channel = np.stack(
        [(GROUP // near) * (source % near) + source // near + rows * c for c in range(2)]
    )
    freq = np.arange(GROUP)
    phase = 2.0 * np.pi * (freq[:, None, None] * channel[None] % GROUP) / GROUP
    both = np.stack([np.cos(phase), np.sin(phase)], 2)
    return jnp.asarray(both.reshape(GROUP, -1), jnp.bfloat16)


def channels_body(x_ref, table_ref, out_ref, scr):
    scr[...] = x_ref[...].astype(jnp.float32)
    rows = [
        jnp.concatenate([scr[:, 2 * j, :], scr[:, 2 * j + 1, :]], 1).astype(jnp.bfloat16)
        for j in range(4)
    ]
    data = jnp.concatenate(rows, 0)
    spectrum = jnp.dot(table_ref[...], data, preferred_element_type=jnp.float32)
    out_ref[...] = jnp.broadcast_to(spectrum.T.astype(jnp.bfloat16)[None], out_ref.shape)


def channel_mix(arrived, table, copies):
    count = arrived.shape[1] * arrived.shape[2] // 4
    return pl.pallas_call(
        channels_body,
        out_shape=pltpu.VMEM((copies, count, GROUP), jnp.bfloat16),
        scratch_shapes=[pltpu.VMEM(arrived.shape, jnp.float32)],
        compiler_params=SMALL,
    )(arrived, table)


def output_body(half_ref, spec_ref, own_ref, other_ref, out_ref):
    half = half_ref[0]
    groups = spec_ref.shape[0]
    for k in range(2):
        for ref, place in ((own_ref, 2 * half + k), (other_ref, 2 * (1 - half) + k)):
            total = None
            for g in range(groups):
                part = jnp.dot(
                    spec_ref[g],
                    ref[k, GROUP * g : GROUP * g + GROUP, :],
                    preferred_element_type=jnp.float32,
                )
                total = part if total is None else total + part
            out_ref[pl.ds(place, 1)] = total.astype(jnp.bfloat16)[None]


def output_map(half, gathered, own, other):
    count = gathered.shape[1]
    return pl.pallas_call(
        output_body,
        in_specs=[
            pl.BlockSpec(memory_space=pltpu.SMEM),
            pl.BlockSpec(memory_space=pltpu.VMEM),
            pl.BlockSpec(memory_space=pltpu.VMEM),
            pl.BlockSpec(memory_space=pltpu.VMEM),
        ],
        out_shape=pltpu.VMEM((4, count, own.shape[2]), jnp.bfloat16),
        compiler_params=SMALL,
    )(half, gathered, own, other)


def local(tokens, norm_gain, w_in, w_out):
    rows = lax.axis_size("row")
    total = tokens.shape[0] * rows
    own = lax.all_gather(w_out, "k", axis=0)
    other = lax.ppermute(own, "h", [(0, 1), (1, 0)])
    projected = project(tokens, w_in, norm_gain)
    arrived = lax.all_to_all(projected, "row", 0, 0, tiled=True)
    spectra = positions(arrived, total)
    arrived = lax.all_to_all(spectra, ("row", "h", "k"), 0, 0, tiled=True)
    mixed = channel_mix(arrived, channel_table(rows, 4), 4)
    gathered = lax.all_to_all(mixed, "g", 0, 0, tiled=True)
    half = lax.axis_index("h").astype(jnp.int32).reshape(1)
    output = output_map(half, gathered, own, other)
    output = lax.all_to_all(output, ("h", "k"), 0, 0, tiled=True)
    return output.reshape(tokens.shape[0], w_out.shape[1])


def solution(mesh):
    mesh = Mesh(mesh.devices.reshape(32, 4, 2, 2), ("row", "g", "h", "k"))
    columns = ("g", "h", "k")
    placed = (P("row", None), P(), P(None, columns), P(None, columns))
    return jax.shard_map(
        local, mesh=mesh, in_specs=placed, out_specs=P("row", columns), check_vma=False
    )
```

```python
import math

import jax
import jax.numpy as jnp
import numpy as np
from jax import lax
from jax.experimental import pallas as pl
from jax.experimental.pallas import tpu as pltpu
from jax.sharding import Mesh
from jax.sharding import PartitionSpec as P

GROUP = 256
NORM_EPS = 1e-06
BLOCK = 128
AHEAD = 3
SMALL = pltpu.CompilerParams(vmem_limit_bytes=16 << 20)


def project_body(x_hbm, w_hbm, gain_hbm, out_ref, x_buf, w_buf, gain_buf, scr, sems):
    pieces = sems.shape[0] - 2
    rows = x_buf.shape[0] // pieces
    weights = pltpu.make_async_copy(w_hbm, w_buf, sems.at[pieces])
    gains = pltpu.make_async_copy(gain_hbm, gain_buf, sems.at[pieces + 1])
    weights.start()
    gains.start()
    copies = []
    for j in range(pieces):
        span = pl.ds(rows * j, rows)
        copies.append(pltpu.make_async_copy(x_hbm.at[span], x_buf.at[span], sems.at[j]))
    for j in range(AHEAD):
        copies[j].start()
    weights.wait()
    gains.wait()
    weight = (w_buf[...].astype(jnp.float32) * gain_buf[...]).T.astype(jnp.bfloat16)
    half = weight.shape[1] // 2
    blocks = x_buf.shape[0] // BLOCK


    def finish(j, part, square):
        turned = (part * lax.rsqrt(square + NORM_EPS)).T
        for b in range(rows // BLOCK):
            for c in range(2):
                place = rows // BLOCK * j + b + blocks * c
                scr[:, place, :] = turned[half * c : half * c + half, BLOCK * b : BLOCK * b + BLOCK]

    waiting = None
    for j in range(pieces):
        copies[j].wait()
        if j + AHEAD < pieces:
            copies[j + AHEAD].start()
        x = x_buf[rows * j : rows * j + rows, :]
        wide = x.astype(jnp.float32)
        square = jnp.mean(wide * wide, axis=1, keepdims=True)
        part = jnp.dot(x, weight, preferred_element_type=jnp.float32)
        if waiting is not None:
            finish(*waiting)
        waiting = (j, part, square)
    finish(*waiting)
    out_ref[...] = scr[...].astype(jnp.bfloat16)


def project(tokens, w_in, gain):
    rows, width = tokens.shape
    channels = w_in.shape[1]
    pieces = 4
    shape = (channels // 2, 2 * rows // BLOCK, BLOCK)
    inputs = [
        pltpu.with_memory_space_constraint(a, pltpu.HBM) for a in (tokens, w_in.T, gain[None])
    ]
    return pl.pallas_call(
        project_body,
        in_specs=[pl.BlockSpec(memory_space=pltpu.HBM)] * 3,
        out_specs=pl.BlockSpec(memory_space=pltpu.VMEM),
        out_shape=pltpu.VMEM(shape, jnp.bfloat16),
        scratch_shapes=[
            pltpu.VMEM((rows, width), jnp.bfloat16),
            pltpu.VMEM((channels, width), jnp.bfloat16),
            pltpu.VMEM((1, width), jnp.float32),
            pltpu.VMEM(shape, jnp.float32),
            pltpu.SemaphoreType.DMA((pieces + 2,)),
        ],
        compiler_params=pltpu.CompilerParams(vmem_limit_bytes=24 << 20),
    )(*inputs)


def fft_tables(total, n_first, n_second):
    scale = 1.0 / math.sqrt(total * GROUP)
    one = np.arange(n_first)
    two = np.arange(n_second)
    first = 2.0 * np.pi * (np.outer(one, one) % n_first) / n_first
    table_one = np.concatenate([np.cos(first), np.sin(first)], 0)
    turn = 2.0 * np.pi * np.outer(one, two) / total
    turns = np.stack([np.cos(turn), np.sin(turn)]) * scale
    second = 2.0 * np.pi * (np.outer(two, two) % n_second) / n_second
    cosine, sine = np.cos(second), np.sin(second)
    table_two = np.block([[cosine, sine], [-sine, cosine]])
    return (
        jnp.asarray(table_one, jnp.bfloat16),
        jnp.asarray(turns, jnp.float32),
        jnp.asarray(table_two, jnp.bfloat16),
    )


def positions_body(x_ref, one_ref, turn_ref, two_ref, out_ref, scr):
    wide = x_ref[...].astype(jnp.float32)
    n_first = wide.shape[0] * 8
    both = [
        wide[:, 8 * c : 8 * c + 8, :].reshape(n_first, BLOCK).astype(jnp.bfloat16)
        for c in range(2)
    ]
    cosine, sine = turn_ref[0], turn_ref[1]
    for c in range(2):
        y = jnp.dot(one_ref[...], both[c], preferred_element_type=jnp.float32)
        y_cos, y_sin = y[:n_first], y[n_first:]
        turned = jnp.concatenate(
            [y_cos * cosine - y_sin * sine, -(y_sin * cosine) - y_cos * sine], 1
        ).astype(jnp.bfloat16)
        z = lax.dot_general(
            two_ref[...], turned, (((1,), (1,)), ((), ())), preferred_element_type=jnp.float32
        )
        for part in range(2):
            for high in range(2):
                scr[:, 4 * c + 2 * part + high, :] = z[
                    BLOCK * part : BLOCK * part + BLOCK, BLOCK * high : BLOCK * high + BLOCK
                ]
    out_ref[...] = scr[...].astype(jnp.bfloat16)


def positions(arrived, total):
    rows = arrived.shape[0]
    tables = fft_tables(total, rows * 8, BLOCK)
    shape = (BLOCK, 8, BLOCK)
    return pl.pallas_call(
        positions_body,
        out_shape=pltpu.VMEM(shape, jnp.bfloat16),
        scratch_shapes=[pltpu.VMEM(shape, jnp.float32)],
        compiler_params=SMALL,
    )(arrived, *tables)


def channel_table(rows, near):
    source = np.arange(rows * near)
    channel = np.stack(
        [(GROUP // near) * (source % near) + source // near + rows * c for c in range(2)]
    )
    freq = np.arange(GROUP)
    phase = 2.0 * np.pi * (freq[:, None, None] * channel[None] % GROUP) / GROUP
    both = np.stack([np.cos(phase), np.sin(phase)], 2)
    return jnp.asarray(both.reshape(GROUP, -1), jnp.bfloat16)


def channels_body(x_ref, table_ref, out_ref, scr):
    scr[...] = x_ref[...].astype(jnp.float32)
    rows = [
        jnp.concatenate([scr[:, 2 * j, :], scr[:, 2 * j + 1, :]], 1).astype(jnp.bfloat16)
        for j in range(4)
    ]
    data = jnp.concatenate(rows, 0)
    spectrum = jnp.dot(table_ref[...], data, preferred_element_type=jnp.float32)
    out_ref[...] = jnp.broadcast_to(spectrum.T.astype(jnp.bfloat16)[None], out_ref.shape)


def channel_mix(arrived, table, copies):
    count = arrived.shape[1] * arrived.shape[2] // 4
    return pl.pallas_call(
        channels_body,
        out_shape=pltpu.VMEM((copies, count, GROUP), jnp.bfloat16),
        scratch_shapes=[pltpu.VMEM(arrived.shape, jnp.float32)],
        compiler_params=SMALL,
    )(arrived, table)


def output_body(half_ref, spec_ref, own_ref, other_ref, out_ref):
    half = half_ref[0]
    groups = spec_ref.shape[0]
    for k in range(2):
        for ref, place in ((own_ref, 2 * half + k), (other_ref, 2 * (1 - half) + k)):
            total = None
            for g in range(groups):
                part = jnp.dot(
                    spec_ref[g],
                    ref[k, GROUP * g : GROUP * g + GROUP, :],
                    preferred_element_type=jnp.float32,
                )
                total = part if total is None else total + part
            out_ref[pl.ds(place, 1)] = total.astype(jnp.bfloat16)[None]


def output_map(half, gathered, own, other):
    count = gathered.shape[1]
    return pl.pallas_call(
        output_body,
        in_specs=[
            pl.BlockSpec(memory_space=pltpu.SMEM),
            pl.BlockSpec(memory_space=pltpu.VMEM),
            pl.BlockSpec(memory_space=pltpu.VMEM),
            pl.BlockSpec(memory_space=pltpu.VMEM),
        ],
        out_shape=pltpu.VMEM((4, count, own.shape[2]), jnp.bfloat16),
        compiler_params=SMALL,
    )(half, gathered, own, other)


def local(tokens, norm_gain, w_in, w_out):
    rows = lax.axis_size("row")
    total = tokens.shape[0] * rows
    own = lax.all_gather(w_out, "k", axis=0)
    other = lax.ppermute(own, "h", [(0, 1), (1, 0)])
    projected = project(tokens, w_in, norm_gain)
    arrived = lax.all_to_all(projected, "row", 0, 0, tiled=True)
    spectra = positions(arrived, total)
    arrived = lax.all_to_all(spectra, ("row", "h", "k"), 0, 0, tiled=True)
    half = lax.axis_index("h").astype(jnp.int32).reshape(1)
    arrived, own, other, half = lax.optimization_barrier((arrived, own, other, half))
    mixed = channel_mix(arrived, channel_table(rows, 4), 4)
    gathered = lax.all_to_all(mixed, "g", 0, 0, tiled=True)
    output = output_map(half, gathered, own, other)
    output = lax.all_to_all(output, ("h", "k"), 0, 0, tiled=True)
    return output.reshape(tokens.shape[0], w_out.shape[1])


def solution(mesh):
    mesh = Mesh(mesh.devices.reshape(32, 4, 2, 2), ("row", "g", "h", "k"))
    columns = ("g", "h", "k")
    placed = (P("row", None), P(), P(None, columns), P(None, columns))
    return jax.shard_map(
        local, mesh=mesh, in_specs=placed, out_specs=P("row", columns), check_vma=False
    )
```

```python
import math

import jax
import jax.numpy as jnp
import numpy as np
from jax import lax
from jax.experimental import pallas as pl
from jax.experimental.pallas import tpu as pltpu
from jax.sharding import Mesh
from jax.sharding import PartitionSpec as P

GROUP = 256
NORM_EPS = 1e-06
BLOCK = 128
AHEAD = 3
SMALL = pltpu.CompilerParams(vmem_limit_bytes=16 << 20)


def project_body(x_hbm, w_hbm, gain_hbm, out_ref, x_buf, w_buf, gain_buf, scr, sems):
    pieces = sems.shape[0] - 2
    rows = x_buf.shape[0] // pieces
    weights = pltpu.make_async_copy(w_hbm, w_buf, sems.at[pieces])
    gains = pltpu.make_async_copy(gain_hbm, gain_buf, sems.at[pieces + 1])
    weights.start()
    gains.start()
    copies = []
    for j in range(pieces):
        span = pl.ds(rows * j, rows)
        copies.append(pltpu.make_async_copy(x_hbm.at[span], x_buf.at[span], sems.at[j]))
    for j in range(AHEAD):
        copies[j].start()
    weights.wait()
    gains.wait()
    weight = (w_buf[...].astype(jnp.float32) * gain_buf[...]).T.astype(jnp.bfloat16)
    half = weight.shape[1] // 2
    blocks = x_buf.shape[0] // BLOCK


    def finish(j, part, square):
        turned = (part * lax.rsqrt(square + NORM_EPS)).T
        for b in range(rows // BLOCK):
            for c in range(2):
                place = rows // BLOCK * j + b + blocks * c
                scr[:, place, :] = turned[half * c : half * c + half, BLOCK * b : BLOCK * b + BLOCK]

    waiting = None
    for j in range(pieces):
        copies[j].wait()
        if j + AHEAD < pieces:
            copies[j + AHEAD].start()
        x = x_buf[rows * j : rows * j + rows, :]
        wide = x.astype(jnp.float32)
        square = jnp.mean(wide * wide, axis=1, keepdims=True)
        part = jnp.dot(x, weight, preferred_element_type=jnp.float32)
        if waiting is not None:
            finish(*waiting)
        waiting = (j, part, square)
    finish(*waiting)
    out_ref[...] = scr[...].astype(jnp.bfloat16)


def project(tokens, w_in, gain):
    rows, width = tokens.shape
    channels = w_in.shape[1]
    pieces = 4
    shape = (channels // 2, 2 * rows // BLOCK, BLOCK)
    inputs = [
        pltpu.with_memory_space_constraint(a, pltpu.HBM) for a in (tokens, w_in.T, gain[None])
    ]
    return pl.pallas_call(
        project_body,
        in_specs=[pl.BlockSpec(memory_space=pltpu.HBM)] * 3,
        out_specs=pl.BlockSpec(memory_space=pltpu.VMEM),
        out_shape=pltpu.VMEM(shape, jnp.bfloat16),
        scratch_shapes=[
            pltpu.VMEM((rows, width), jnp.bfloat16),
            pltpu.VMEM((channels, width), jnp.bfloat16),
            pltpu.VMEM((1, width), jnp.float32),
            pltpu.VMEM(shape, jnp.float32),
            pltpu.SemaphoreType.DMA((pieces + 2,)),
        ],
        compiler_params=pltpu.CompilerParams(vmem_limit_bytes=24 << 20),
    )(*inputs)


def fft_tables(total, n_first, n_second):
    scale = 1.0 / math.sqrt(total * GROUP)
    one = np.arange(n_first)
    two = np.arange(n_second)
    first = 2.0 * np.pi * (np.outer(one, one) % n_first) / n_first
    table_one = np.concatenate([np.cos(first), np.sin(first)], 0)
    turn = 2.0 * np.pi * np.outer(one, two) / total
    turns = np.stack([np.cos(turn), np.sin(turn)]) * scale
    second = 2.0 * np.pi * (np.outer(two, two) % n_second) / n_second
    cosine, sine = np.cos(second), np.sin(second)
    table_two = np.block([[cosine, sine], [-sine, cosine]])
    return (
        jnp.asarray(table_one, jnp.bfloat16),
        jnp.asarray(turns, jnp.float32),
        jnp.asarray(table_two, jnp.bfloat16),
    )


def positions_body(x_ref, one_ref, turn_ref, two_ref, out_ref, scr):
    wide = x_ref[...].astype(jnp.float32)
    n_first = wide.shape[0] * 8
    both = [
        wide[:, 8 * c : 8 * c + 8, :].reshape(n_first, BLOCK).astype(jnp.bfloat16)
        for c in range(2)
    ]
    cosine, sine = turn_ref[0], turn_ref[1]
    for c in range(2):
        y = jnp.dot(one_ref[...], both[c], preferred_element_type=jnp.float32)
        y_cos, y_sin = y[:n_first], y[n_first:]
        turned = jnp.concatenate(
            [y_cos * cosine - y_sin * sine, -(y_sin * cosine) - y_cos * sine], 1
        ).astype(jnp.bfloat16)
        z = lax.dot_general(
            two_ref[...], turned, (((1,), (1,)), ((), ())), preferred_element_type=jnp.float32
        )
        for part in range(2):
            for high in range(2):
                scr[:, 4 * c + 2 * part + high, :] = z[
                    BLOCK * part : BLOCK * part + BLOCK, BLOCK * high : BLOCK * high + BLOCK
                ]
    out_ref[...] = scr[...].astype(jnp.bfloat16)


def positions(arrived, total):
    rows = arrived.shape[0]
    tables = fft_tables(total, rows * 8, BLOCK)
    shape = (BLOCK, 8, BLOCK)
    return pl.pallas_call(
        positions_body,
        out_shape=pltpu.VMEM(shape, jnp.bfloat16),
        scratch_shapes=[pltpu.VMEM(shape, jnp.float32)],
        compiler_params=SMALL,
    )(arrived, *tables)


def channel_table(rows):
    source = np.arange(4 * rows)
    core, row, half = source // (2 * rows), source // 2 % rows, source % 2
    place = 2 * half + core
    channel = np.stack([GROUP // 4 * place + row + rows * c for c in range(2)])
    freq = np.arange(GROUP)
    phase = 2.0 * np.pi * (freq[:, None, None] * channel[None] % GROUP) / GROUP
    both = np.stack([np.cos(phase), np.sin(phase)], 2)
    return jnp.asarray(both.reshape(GROUP, -1), jnp.bfloat16)


def channels_body(core_ref, x_ref, table_ref, out_ref, scr):
    core = core_ref[0]
    for k in range(2):
        part = x_ref[k, :, pl.ds(core, 1)]
        count = part.shape[0]
        scr[count * k : count * k + count] = part.reshape(count, *scr.shape[1:]).astype(jnp.float32)
    rows = [
        jnp.concatenate([scr[:, 2 * j, :], scr[:, 2 * j + 1, :]], 1).astype(jnp.bfloat16)
        for j in range(4)
    ]
    data = jnp.concatenate(rows, 0)
    spectrum = jnp.dot(table_ref[...], data, preferred_element_type=jnp.float32)
    out_ref[...] = spectrum.T.astype(jnp.bfloat16)


def channel_mix(core, arrived, table):
    sources, height, width = arrived.shape[1], *arrived.shape[3:]
    return pl.pallas_call(
        channels_body,
        in_specs=[
            pl.BlockSpec(memory_space=pltpu.SMEM),
            pl.BlockSpec(memory_space=pltpu.VMEM),
            pl.BlockSpec(memory_space=pltpu.VMEM),
        ],
        out_shape=pltpu.VMEM((height * width // 4, GROUP), jnp.bfloat16),
        scratch_shapes=[pltpu.VMEM((2 * sources, height, width), jnp.float32)],
        compiler_params=SMALL,
    )(core, arrived, table)


def output_body(half_ref, spec_ref, own_ref, other_ref, out_ref):
    half = half_ref[0]
    groups = spec_ref.shape[0]
    for k in range(2):
        for ref, place in ((own_ref, 2 * half + k), (other_ref, 2 * (1 - half) + k)):
            total = None
            for g in range(groups):
                part = jnp.dot(
                    spec_ref[g],
                    ref[k, GROUP * g : GROUP * g + GROUP, :],
                    preferred_element_type=jnp.float32,
                )
                total = part if total is None else total + part
            out_ref[pl.ds(place, 1)] = total.astype(jnp.bfloat16)[None]


def output_map(half, gathered, own, other):
    count = gathered.shape[1]
    return pl.pallas_call(
        output_body,
        in_specs=[
            pl.BlockSpec(memory_space=pltpu.SMEM),
            pl.BlockSpec(memory_space=pltpu.VMEM),
            pl.BlockSpec(memory_space=pltpu.VMEM),
            pl.BlockSpec(memory_space=pltpu.VMEM),
        ],
        out_shape=pltpu.VMEM((4, count, own.shape[2]), jnp.bfloat16),
        compiler_params=SMALL,
    )(half, gathered, own, other)


def local(tokens, norm_gain, w_in, w_out):
    rows = lax.axis_size("row")
    total = tokens.shape[0] * rows
    own = lax.all_gather(w_out, "k", axis=0)
    other = lax.ppermute(own, "h", [(0, 1), (1, 0)])
    projected = project(tokens, w_in, norm_gain)
    arrived = lax.all_to_all(projected, "row", 0, 0, tiled=True)
    spectra = positions(arrived, total)
    arrived = lax.all_to_all(spectra, ("row", "h"), 0, 0, tiled=True)
    arrived = lax.all_gather(arrived.reshape(2 * rows, 2, *arrived.shape[1:]), "k", axis=0)
    core = lax.axis_index("k").astype(jnp.int32).reshape(1)
    mixed = channel_mix(core, arrived, channel_table(rows))
    gathered = lax.all_gather(mixed, "g", axis=0)
    half = lax.axis_index("h").astype(jnp.int32).reshape(1)
    output = output_map(half, gathered, own, other)
    output = lax.all_to_all(output, ("h", "k"), 0, 0, tiled=True)
    return output.reshape(tokens.shape[0], w_out.shape[1])


def solution(mesh):
    mesh = Mesh(mesh.devices.reshape(32, 4, 2, 2), ("row", "g", "h", "k"))
    columns = ("g", "h", "k")
    placed = (P("row", None), P(), P(None, columns), P(None, columns))
    return jax.shard_map(
        local, mesh=mesh, in_specs=placed, out_specs=P("row", columns), check_vma=False
    )
```

```python
import math

import jax
import jax.numpy as jnp
import numpy as np
from jax import lax
from jax.experimental import pallas as pl
from jax.experimental.pallas import tpu as pltpu
from jax.sharding import Mesh
from jax.sharding import PartitionSpec as P


GROUP = 256
NORM_EPS = 1e-06
BLOCK = 128
AHEAD = 3
SMALL = pltpu.CompilerParams(vmem_limit_bytes=16 << 20)


def project_body(x_hbm, w_hbm, gain_hbm, out_ref, x_buf, w_buf, gain_buf, scr, sems):
    pieces = sems.shape[0] - 2
    rows = x_buf.shape[0] // pieces
    weights = pltpu.make_async_copy(w_hbm, w_buf, sems.at[pieces])
    gains = pltpu.make_async_copy(gain_hbm, gain_buf, sems.at[pieces + 1])
    weights.start()
    gains.start()
    copies = []
    for j in range(pieces):
        span = pl.ds(rows * j, rows)
        copies.append(pltpu.make_async_copy(x_hbm.at[span], x_buf.at[span], sems.at[j]))
    for j in range(AHEAD):
        copies[j].start()
    weights.wait()
    gains.wait()
    weight = (w_buf[...].astype(jnp.float32) * gain_buf[...]).T.astype(jnp.bfloat16)
    half = weight.shape[1] // 2
    blocks = x_buf.shape[0] // BLOCK


    def finish(j, part, square):
        turned = (part * lax.rsqrt(square + NORM_EPS)).T
        for b in range(rows // BLOCK):
            for c in range(2):
                place = rows // BLOCK * j + b + blocks * c
                scr[:, place, :] = turned[half * c : half * c + half, BLOCK * b : BLOCK * b + BLOCK]

    waiting = None
    for j in range(pieces):
        copies[j].wait()
        if j + AHEAD < pieces:
            copies[j + AHEAD].start()
        x = x_buf[rows * j : rows * j + rows, :]
        wide = x.astype(jnp.float32)
        square = jnp.mean(wide * wide, axis=1, keepdims=True)
        part = jnp.dot(x, weight, preferred_element_type=jnp.float32)
        if waiting is not None:
            finish(*waiting)
        waiting = (j, part, square)
    finish(*waiting)
    out_ref[...] = scr[...].astype(jnp.bfloat16)


def project(tokens, w_in, gain):
    rows, width = tokens.shape
    channels = w_in.shape[1]
    pieces = 4
    shape = (channels // 2, 2 * rows // BLOCK, BLOCK)
    inputs = [
        pltpu.with_memory_space_constraint(a, pltpu.HBM) for a in (tokens, w_in.T, gain[None])
    ]
    return pl.pallas_call(
        project_body,
        in_specs=[pl.BlockSpec(memory_space=pltpu.HBM)] * 3,
        out_specs=pl.BlockSpec(memory_space=pltpu.VMEM),
        out_shape=pltpu.VMEM(shape, jnp.bfloat16),
        scratch_shapes=[
            pltpu.VMEM((rows, width), jnp.bfloat16),
            pltpu.VMEM((channels, width), jnp.bfloat16),
            pltpu.VMEM((1, width), jnp.float32),
            pltpu.VMEM(shape, jnp.float32),
            pltpu.SemaphoreType.DMA((pieces + 2,)),
        ],
        compiler_params=pltpu.CompilerParams(vmem_limit_bytes=24 << 20),
    )(*inputs)


def fft_tables(total, n_first, n_second):
    scale = 1.0 / math.sqrt(total * GROUP)
    one = np.arange(n_first)
    two = np.arange(n_second)
    first = 2.0 * np.pi * (np.outer(one, one) % n_first) / n_first
    table_one = np.concatenate([np.cos(first), np.sin(first)], 0)
    turn = 2.0 * np.pi * np.outer(one, two) / total
    turns = np.stack([np.cos(turn), np.sin(turn)]) * scale
    second = 2.0 * np.pi * (np.outer(two, two) % n_second) / n_second
    cosine, sine = np.cos(second), np.sin(second)
    table_two = np.block([[cosine, sine], [-sine, cosine]])
    return (
        jnp.asarray(table_one, jnp.bfloat16),
        jnp.asarray(turns, jnp.float32),
        jnp.asarray(table_two, jnp.bfloat16),
    )


def positions_body(x_ref, one_ref, turn_ref, two_ref, out_ref, scr):
    wide = x_ref[...].astype(jnp.float32)
    n_first = wide.shape[0] * 8
    both = [
        wide[:, 8 * c : 8 * c + 8, :].reshape(n_first, BLOCK).astype(jnp.bfloat16)
        for c in range(2)
    ]
    cosine, sine = turn_ref[0], turn_ref[1]
    for c in range(2):
        y = jnp.dot(one_ref[...], both[c], preferred_element_type=jnp.float32)
        y_cos, y_sin = y[:n_first], y[n_first:]
        turned = jnp.concatenate(
            [y_cos * cosine - y_sin * sine, -(y_sin * cosine) - y_cos * sine], 1
        ).astype(jnp.bfloat16)
        z = lax.dot_general(
            two_ref[...], turned, (((1,), (1,)), ((), ())), preferred_element_type=jnp.float32
        )
        for part in range(2):
            for high in range(2):
                scr[:, 4 * c + 2 * part + high, :] = z[
                    BLOCK * part : BLOCK * part + BLOCK, BLOCK * high : BLOCK * high + BLOCK
                ]
    out_ref[...] = scr[...].astype(jnp.bfloat16)


def positions(arrived, total):
    rows = arrived.shape[0]
    tables = fft_tables(total, rows * 8, BLOCK)
    shape = (BLOCK, 8, BLOCK)
    return pl.pallas_call(
        positions_body,
        out_shape=pltpu.VMEM(shape, jnp.bfloat16),
        scratch_shapes=[pltpu.VMEM(shape, jnp.float32)],
        compiler_params=SMALL,
    )(arrived, *tables)


def channel_table(rows):
    source = np.arange(4 * rows)
    core, row, half = source // (2 * rows), source // 2 % rows, source % 2
    place = 2 * half + core
    channel = np.stack([GROUP // 4 * place + row + rows * c for c in range(2)])
    freq = np.arange(GROUP)
    phase = 2.0 * np.pi * (freq[:, None, None] * channel[None] % GROUP) / GROUP
    both = np.stack([np.cos(phase), np.sin(phase)], 2)
    return jnp.asarray(both.reshape(GROUP, -1), jnp.bfloat16)


def channels_body(core_ref, x_ref, table_ref, out_ref, scr):
    core = core_ref[0]
    for k in range(2):
        part = x_ref[k, :, pl.ds(core, 1)]
        count = part.shape[0]
        scr[count * k : count * k + count] = part.reshape(count, *scr.shape[1:]).astype(jnp.float32)
    rows = [
        jnp.concatenate([scr[:, 2 * j, :], scr[:, 2 * j + 1, :]], 1).astype(jnp.bfloat16)
        for j in range(4)
    ]
    data = jnp.concatenate(rows, 0)
    spectrum = jnp.dot(table_ref[...], data, preferred_element_type=jnp.float32)
    out_ref[...] = spectrum.T.astype(jnp.bfloat16)


def channel_mix(core, arrived, table):
    sources, height, width = arrived.shape[1], *arrived.shape[3:]
    return pl.pallas_call(
        channels_body,
        in_specs=[
            pl.BlockSpec(memory_space=pltpu.SMEM),
            pl.BlockSpec(memory_space=pltpu.VMEM),
            pl.BlockSpec(memory_space=pltpu.VMEM),
        ],
        out_shape=pltpu.VMEM((height * width // 4, GROUP), jnp.bfloat16),
        scratch_shapes=[pltpu.VMEM((2 * sources, height, width), jnp.float32)],
        compiler_params=SMALL,
    )(core, arrived, table)


def output_body(half_ref, spec_ref, own_ref, other_ref, out_ref):
    half = half_ref[0]
    groups = spec_ref.shape[0]
    for k in range(2):
        for ref, place in ((own_ref, 2 * half + k), (other_ref, 2 * (1 - half) + k)):
            total = None
            for g in range(groups):
                part = jnp.dot(
                    spec_ref[g],
                    ref[k, GROUP * g : GROUP * g + GROUP, :],
                    preferred_element_type=jnp.float32,
                )
                total = part if total is None else total + part
            out_ref[pl.ds(place, 1)] = total.astype(jnp.bfloat16)[None]


def output_map(half, gathered, own, other):
    count = gathered.shape[1]
    return pl.pallas_call(
        output_body,
        in_specs=[
            pl.BlockSpec(memory_space=pltpu.SMEM),
            pl.BlockSpec(memory_space=pltpu.VMEM),
            pl.BlockSpec(memory_space=pltpu.VMEM),
            pl.BlockSpec(memory_space=pltpu.VMEM),
        ],
        out_shape=pltpu.VMEM((4, count, own.shape[2]), jnp.bfloat16),
        compiler_params=SMALL,
    )(half, gathered, own, other)


def local(tokens, norm_gain, w_in, w_out):
    rows = lax.axis_size("row")
    total = tokens.shape[0] * rows
    other = lax.ppermute(w_out, "h", [(0, 1), (1, 0)])
    own = lax.all_gather(w_out, "k", axis=0)
    other = lax.all_gather(other, "k", axis=0)
    projected = project(tokens, w_in, norm_gain)
    arrived = lax.all_to_all(projected, "row", 0, 0, tiled=True)
    half, core = (lax.axis_index(name).astype(jnp.int32).reshape(1) for name in ("h", "k"))
    arrived, half, core = lax.optimization_barrier((arrived, half, core))
    spectra = positions(arrived, total)
    arrived = lax.all_to_all(spectra, ("row", "h"), 0, 0, tiled=True)
    arrived = lax.all_gather(arrived.reshape(2 * rows, 2, *arrived.shape[1:]), "k", axis=0)
    mixed = channel_mix(core, arrived, channel_table(rows))
    gathered = lax.all_gather(mixed, "g", axis=0)
    output = output_map(half, gathered, own, other)
    output = lax.all_to_all(output, ("h", "k"), 0, 0, tiled=True)
    return output.reshape(tokens.shape[0], w_out.shape[1])


def solution(mesh):
    mesh = Mesh(mesh.devices.reshape(32, 4, 2, 2), ("row", "g", "h", "k"))
    columns = ("g", "h", "k")
    placed = (P("row", None), P(), P(None, columns), P(None, columns))
    return jax.shard_map(
        local, mesh=mesh, in_specs=placed, out_specs=P("row", columns), check_vma=False
    )
```

```python
import math

import jax
import jax.numpy as jnp
import numpy as np
from jax import lax
from jax.experimental import pallas as pl
from jax.experimental.pallas import tpu as pltpu
from jax.sharding import Mesh
from jax.sharding import PartitionSpec as P


GROUP = 256
NORM_EPS = 1e-06
BLOCK = 128
AHEAD = 3
SMALL = pltpu.CompilerParams(vmem_limit_bytes=16 << 20)


def project_body(x_hbm, w_hbm, gain_hbm, out_ref, x_buf, w_buf, gain_buf, scr, sems):
    pieces = sems.shape[0] - 2
    rows = x_buf.shape[0] // pieces
    weights = pltpu.make_async_copy(w_hbm, w_buf, sems.at[pieces])
    gains = pltpu.make_async_copy(gain_hbm, gain_buf, sems.at[pieces + 1])
    weights.start()
    gains.start()
    copies = []
    for j in range(pieces):
        span = pl.ds(rows * j, rows)
        copies.append(pltpu.make_async_copy(x_hbm.at[span], x_buf.at[span], sems.at[j]))
    for j in range(AHEAD):
        copies[j].start()
    weights.wait()
    gains.wait()
    weight = (w_buf[...].astype(jnp.float32) * gain_buf[...]).T.astype(jnp.bfloat16)
    half = weight.shape[1] // 2
    blocks = x_buf.shape[0] // BLOCK


    def finish(j, part, square):
        turned = (part * lax.rsqrt(square + NORM_EPS)).T
        for b in range(rows // BLOCK):
            for c in range(2):
                place = rows // BLOCK * j + b + blocks * c
                scr[:, place, :] = turned[half * c : half * c + half, BLOCK * b : BLOCK * b + BLOCK]

    waiting = None
    for j in range(pieces):
        copies[j].wait()
        if j + AHEAD < pieces:
            copies[j + AHEAD].start()
        x = x_buf[rows * j : rows * j + rows, :]
        wide = x.astype(jnp.float32)
        square = jnp.mean(wide * wide, axis=1, keepdims=True)
        part = jnp.dot(x, weight, preferred_element_type=jnp.float32)
        if waiting is not None:
            finish(*waiting)
        waiting = (j, part, square)
    finish(*waiting)
    out_ref[...] = scr[...].astype(jnp.bfloat16)


def project(tokens, w_in, gain):
    rows, width = tokens.shape
    channels = w_in.shape[1]
    pieces = 4
    shape = (channels // 2, 2 * rows // BLOCK, BLOCK)
    inputs = [
        pltpu.with_memory_space_constraint(a, pltpu.HBM) for a in (tokens, w_in.T, gain[None])
    ]
    return pl.pallas_call(
        project_body,
        in_specs=[pl.BlockSpec(memory_space=pltpu.HBM)] * 3,
        out_specs=pl.BlockSpec(memory_space=pltpu.VMEM),
        out_shape=pltpu.VMEM(shape, jnp.bfloat16),
        scratch_shapes=[
            pltpu.VMEM((rows, width), jnp.bfloat16),
            pltpu.VMEM((channels, width), jnp.bfloat16),
            pltpu.VMEM((1, width), jnp.float32),
            pltpu.VMEM(shape, jnp.float32),
            pltpu.SemaphoreType.DMA((pieces + 2,)),
        ],
        compiler_params=pltpu.CompilerParams(vmem_limit_bytes=24 << 20),
    )(*inputs)


def fft_tables(total, n_first, n_second):
    scale = 1.0 / math.sqrt(total * GROUP)
    one = np.arange(n_first)
    two = np.arange(n_second)
    first = 2.0 * np.pi * (np.outer(one, one) % n_first) / n_first
    table_one = np.concatenate([np.cos(first), np.sin(first)], 0)
    turn = 2.0 * np.pi * np.outer(one, two) / total
    turns = np.stack([np.cos(turn), np.sin(turn)]) * scale
    second = 2.0 * np.pi * (np.outer(two, two) % n_second) / n_second
    cosine, sine = np.cos(second), np.sin(second)
    table_two = np.block([[cosine, sine], [-sine, cosine]])
    return (
        jnp.asarray(table_one, jnp.bfloat16),
        jnp.asarray(turns, jnp.float32),
        jnp.asarray(table_two, jnp.bfloat16),
    )


def positions_body(x_ref, one_ref, turn_ref, two_ref, out_ref, scr):
    wide = x_ref[...].astype(jnp.float32)
    n_first = wide.shape[0] * 8
    both = [
        wide[:, 8 * c : 8 * c + 8, :].reshape(n_first, BLOCK).astype(jnp.bfloat16)
        for c in range(2)
    ]
    cosine, sine = turn_ref[0], turn_ref[1]
    for c in range(2):
        y = jnp.dot(one_ref[...], both[c], preferred_element_type=jnp.float32)
        y_cos, y_sin = y[:n_first], y[n_first:]
        turned = jnp.concatenate(
            [y_cos * cosine - y_sin * sine, -(y_sin * cosine) - y_cos * sine], 1
        ).astype(jnp.bfloat16)
        z = lax.dot_general(
            two_ref[...], turned, (((1,), (1,)), ((), ())), preferred_element_type=jnp.float32
        )
        for part in range(2):
            for high in range(2):
                scr[:, 4 * c + 2 * part + high, :] = z[
                    BLOCK * part : BLOCK * part + BLOCK, BLOCK * high : BLOCK * high + BLOCK
                ]
    out_ref[...] = scr[...].astype(jnp.bfloat16)


def positions(arrived, total):
    rows = arrived.shape[0]
    tables = fft_tables(total, rows * 8, BLOCK)
    shape = (BLOCK, 8, BLOCK)
    return pl.pallas_call(
        positions_body,
        out_shape=pltpu.VMEM(shape, jnp.bfloat16),
        scratch_shapes=[pltpu.VMEM(shape, jnp.float32)],
        compiler_params=SMALL,
    )(arrived, *tables)


def channel_table(rows):
    source = np.arange(4 * rows)
    core, row, half = source // (2 * rows), source // 2 % rows, source % 2
    place = 2 * half + core
    channel = np.stack([GROUP // 4 * place + row + rows * c for c in range(2)])
    freq = np.arange(GROUP)
    phase = 2.0 * np.pi * (freq[:, None, None] * channel[None] % GROUP) / GROUP
    both = np.stack([np.cos(phase), np.sin(phase)], 2)
    return jnp.asarray(both.reshape(GROUP, -1), jnp.bfloat16)


def channels_body(core_ref, x_ref, table_ref, out_ref, scr):
    core = core_ref[0]
    for k in range(2):
        part = x_ref[k, :, pl.ds(core, 1)]
        count = 2 * part.shape[0]
        scr[count * k : count * k + count] = part.reshape(count, *scr.shape[1:]).astype(jnp.float32)
    rows = [
        jnp.concatenate([scr[:, 2 * j, :], scr[:, 2 * j + 1, :]], 1).astype(jnp.bfloat16)
        for j in range(4)
    ]
    data = jnp.concatenate(rows, 0)
    spectrum = jnp.dot(table_ref[...], data, preferred_element_type=jnp.float32)
    out_ref[...] = spectrum.T.astype(jnp.bfloat16)


def channel_mix(core, arrived, table):
    sources, height, width = 2 * arrived.shape[1], *arrived.shape[4:]
    return pl.pallas_call(
        channels_body,
        in_specs=[
            pl.BlockSpec(memory_space=pltpu.SMEM),
            pl.BlockSpec(memory_space=pltpu.VMEM),
            pl.BlockSpec(memory_space=pltpu.VMEM),
        ],
        out_shape=pltpu.VMEM((height * width // 4, GROUP), jnp.bfloat16),
        scratch_shapes=[pltpu.VMEM((2 * sources, height, width), jnp.float32)],
        compiler_params=SMALL,
    )(core, arrived, table)


def output_body(chip_ref, spec_ref, *refs):
    *weights, out_ref = refs
    groups = spec_ref.shape[0]
    for flip, ref in enumerate(weights):
        total = None
        for g in range(groups):
            part = jnp.dot(
                spec_ref[g],
                ref[GROUP * g : GROUP * g + GROUP, :],
                preferred_element_type=jnp.float32,
            )
            total = part if total is None else total + part
        out_ref[pl.ds(chip_ref[0] ^ flip, 1)] = total.astype(jnp.bfloat16)[None]


def output_map(chip, gathered, *weights):
    count = gathered.shape[1]
    whole = pl.BlockSpec(memory_space=pltpu.VMEM)
    return pl.pallas_call(
        output_body,
        in_specs=[pl.BlockSpec(memory_space=pltpu.SMEM)] + [whole] * (1 + len(weights)),
        out_shape=pltpu.VMEM((len(weights), count, weights[0].shape[1]), jnp.bfloat16),
        compiler_params=SMALL,
    )(chip, gathered, *weights)


def local(tokens, norm_gain, w_in, w_out):
    rows = lax.axis_size("row")
    total = tokens.shape[0] * rows
    flips = ((("h",), 1), (("g0",), 1), (("g0", "h"), 3))
    near = [
        lax.ppermute(w_out, axes, [(i, i ^ flip) for i in range(2 * len(axes))])
        for axes, flip in flips
    ]
    projected = project(tokens, w_in, norm_gain)
    arrived = lax.all_to_all(projected, "row", 0, 0, tiled=True)
    spectra = positions(arrived, total)
    arrived = lax.all_to_all(spectra, ("row", "g0", "h"), 0, 0, tiled=True)
    arrived = lax.all_gather(arrived.reshape(rows, 2, 2, *arrived.shape[1:]), "k", axis=0)
    core = lax.axis_index("k").astype(jnp.int32).reshape(1)
    mixed = channel_mix(core, arrived, channel_table(rows))
    gathered = lax.all_gather(mixed, ("g1", "k"), axis=0)
    chip = lax.axis_index(("g0", "h")).astype(jnp.int32).reshape(1)
    output = output_map(chip, gathered, w_out, *near)
    output = lax.all_to_all(output, ("g0", "h"), 0, 0, tiled=True)
    return output.reshape(tokens.shape[0], w_out.shape[1])


def solution(mesh):
    mesh = Mesh(mesh.devices.reshape(32, 2, 2, 2, 2), ("row", "g1", "g0", "h", "k"))
    columns = ("g1", "g0", "h", "k")
    placed = (P("row", None), P(), P(None, columns), P(None, columns))
    return jax.shard_map(
        local, mesh=mesh, in_specs=placed, out_specs=P("row", columns), check_vma=False
    )
```

```python
import math

import jax
import jax.numpy as jnp
import numpy as np
from jax import lax
from jax.experimental import pallas as pl
from jax.experimental.pallas import tpu as pltpu
from jax.sharding import Mesh
from jax.sharding import PartitionSpec as P


GROUP = 256
NORM_EPS = 1e-06
BLOCK = 128
AHEAD = 3
SMALL = pltpu.CompilerParams(vmem_limit_bytes=16 << 20)


def project_body(x_hbm, w_hbm, gain_hbm, out_ref, x_buf, w_buf, gain_buf, scr, sems):
    pieces = sems.shape[0] - 2
    rows = x_buf.shape[0] // pieces
    weights = pltpu.make_async_copy(w_hbm, w_buf, sems.at[pieces])
    gains = pltpu.make_async_copy(gain_hbm, gain_buf, sems.at[pieces + 1])
    weights.start()
    gains.start()
    copies = []
    for j in range(pieces):
        span = pl.ds(rows * j, rows)
        copies.append(pltpu.make_async_copy(x_hbm.at[span], x_buf.at[span], sems.at[j]))
    for j in range(AHEAD):
        copies[j].start()
    weights.wait()
    gains.wait()
    weight = (w_buf[...].astype(jnp.float32) * gain_buf[...]).T.astype(jnp.bfloat16)
    half = weight.shape[1] // 2
    blocks = x_buf.shape[0] // BLOCK


    def finish(j, part, square):
        turned = (part * lax.rsqrt(square + NORM_EPS)).T
        for b in range(rows // BLOCK):
            for c in range(2):
                place = rows // BLOCK * j + b + blocks * c
                scr[:, place, :] = turned[half * c : half * c + half, BLOCK * b : BLOCK * b + BLOCK]

    waiting = None
    for j in range(pieces):
        copies[j].wait()
        if j + AHEAD < pieces:
            copies[j + AHEAD].start()
        x = x_buf[rows * j : rows * j + rows, :]
        wide = x.astype(jnp.float32)
        square = jnp.mean(wide * wide, axis=1, keepdims=True)
        part = jnp.dot(x, weight, preferred_element_type=jnp.float32)
        if waiting is not None:
            finish(*waiting)
        waiting = (j, part, square)
    finish(*waiting)
    out_ref[...] = scr[...].astype(jnp.bfloat16)


def project(tokens, w_in, gain):
    rows, width = tokens.shape
    channels = w_in.shape[1]
    pieces = 4
    shape = (channels // 2, 2 * rows // BLOCK, BLOCK)
    inputs = [
        pltpu.with_memory_space_constraint(a, pltpu.HBM) for a in (tokens, w_in.T, gain[None])
    ]
    return pl.pallas_call(
        project_body,
        in_specs=[pl.BlockSpec(memory_space=pltpu.HBM)] * 3,
        out_specs=pl.BlockSpec(memory_space=pltpu.VMEM),
        out_shape=pltpu.VMEM(shape, jnp.bfloat16),
        scratch_shapes=[
            pltpu.VMEM((rows, width), jnp.bfloat16),
            pltpu.VMEM((channels, width), jnp.bfloat16),
            pltpu.VMEM((1, width), jnp.float32),
            pltpu.VMEM(shape, jnp.float32),
            pltpu.SemaphoreType.DMA((pieces + 2,)),
        ],
        compiler_params=pltpu.CompilerParams(vmem_limit_bytes=24 << 20),
    )(*inputs)


def fft_tables(total, n_first, n_second):
    scale = 1.0 / math.sqrt(total * GROUP)
    one = np.arange(n_first)
    two = np.arange(n_second)
    first = 2.0 * np.pi * (np.outer(one, one) % n_first) / n_first
    table_one = np.concatenate([np.cos(first), np.sin(first)], 0)
    turn = 2.0 * np.pi * np.outer(one, two) / total
    turns = np.stack([np.cos(turn), np.sin(turn)]) * scale
    second = 2.0 * np.pi * (np.outer(two, two) % n_second) / n_second
    cosine, sine = np.cos(second), np.sin(second)
    table_two = np.block([[cosine, sine], [-sine, cosine]])
    return (
        jnp.asarray(table_one, jnp.bfloat16),
        jnp.asarray(turns, jnp.float32),
        jnp.asarray(table_two, jnp.bfloat16),
    )


def positions_body(x_ref, one_ref, turn_ref, two_ref, out_ref, scr):
    wide = x_ref[...].astype(jnp.float32)
    n_first = wide.shape[0] * 8
    both = [
        wide[:, 8 * c : 8 * c + 8, :].reshape(n_first, BLOCK).astype(jnp.bfloat16)
        for c in range(2)
    ]
    cosine, sine = turn_ref[0], turn_ref[1]
    for c in range(2):
        y = jnp.dot(one_ref[...], both[c], preferred_element_type=jnp.float32)
        y_cos, y_sin = y[:n_first], y[n_first:]
        turned = jnp.concatenate(
            [y_cos * cosine - y_sin * sine, -(y_sin * cosine) - y_cos * sine], 1
        ).astype(jnp.bfloat16)
        z = lax.dot_general(
            two_ref[...], turned, (((1,), (1,)), ((), ())), preferred_element_type=jnp.float32
        )
        for part in range(2):
            for high in range(2):
                scr[:, 4 * c + 2 * part + high, :] = z[
                    BLOCK * part : BLOCK * part + BLOCK, BLOCK * high : BLOCK * high + BLOCK
                ]
    out_ref[...] = scr[...].astype(jnp.bfloat16)


def positions(arrived, total):
    rows = arrived.shape[0]
    tables = fft_tables(total, rows * 8, BLOCK)
    shape = (BLOCK, 8, BLOCK)
    return pl.pallas_call(
        positions_body,
        out_shape=pltpu.VMEM(shape, jnp.bfloat16),
        scratch_shapes=[pltpu.VMEM(shape, jnp.float32)],
        compiler_params=SMALL,
    )(arrived, *tables)


def channel_table(rows):
    source = np.arange(4 * rows)
    core, row, half = source // (2 * rows), source // 2 % rows, source % 2
    place = 2 * half + core
    channel = np.stack([GROUP // 4 * place + row + rows * c for c in range(2)])
    freq = np.arange(GROUP)
    phase = 2.0 * np.pi * (freq[:, None, None] * channel[None] % GROUP) / GROUP
    both = np.stack([np.cos(phase), np.sin(phase)], 2)
    return jnp.asarray(both.reshape(GROUP, -1), jnp.bfloat16)


def channels_body(core_ref, x_ref, table_ref, out_ref, scr):
    core = core_ref[0]
    for k in range(2):
        part = x_ref[k, :, pl.ds(core, 1)]
        count = part.shape[0]
        scr[count * k : count * k + count] = part.reshape(count, *scr.shape[1:]).astype(jnp.float32)
    rows = [
        jnp.concatenate([scr[:, 2 * j, :], scr[:, 2 * j + 1, :]], 1).astype(jnp.bfloat16)
        for j in range(4)
    ]
    data = jnp.concatenate(rows, 0)
    spectrum = jnp.dot(table_ref[...], data, preferred_element_type=jnp.float32)
    out_ref[...] = spectrum.T.astype(jnp.bfloat16)


def channel_mix(core, arrived, table):
    sources, height, width = arrived.shape[1], *arrived.shape[3:]
    return pl.pallas_call(
        channels_body,
        in_specs=[
            pl.BlockSpec(memory_space=pltpu.SMEM),
            pl.BlockSpec(memory_space=pltpu.VMEM),
            pl.BlockSpec(memory_space=pltpu.VMEM),
        ],
        out_shape=pltpu.VMEM((height * width // 4, GROUP), jnp.bfloat16),
        scratch_shapes=[pltpu.VMEM((2 * sources, height, width), jnp.float32)],
        compiler_params=SMALL,
    )(core, arrived, table)


def output_body(chip_ref, spec_ref, *refs):
    *weights, out_ref = refs
    groups = spec_ref.shape[0]
    for flip, ref in enumerate(weights):
        total = None
        for g in range(groups):
            part = jnp.dot(
                spec_ref[g],
                ref[GROUP * g : GROUP * g + GROUP, :],
                preferred_element_type=jnp.float32,
            )
            total = part if total is None else total + part
        out_ref[pl.ds(chip_ref[0] ^ flip, 1)] = total.astype(jnp.bfloat16)[None]


def output_map(chip, gathered, *weights):
    count = gathered.shape[1]
    whole = pl.BlockSpec(memory_space=pltpu.VMEM)
    return pl.pallas_call(
        output_body,
        in_specs=[pl.BlockSpec(memory_space=pltpu.SMEM)] + [whole] * (1 + len(weights)),
        out_shape=pltpu.VMEM((len(weights), count, weights[0].shape[1]), jnp.bfloat16),
        compiler_params=SMALL,
    )(chip, gathered, *weights)


def local(tokens, norm_gain, w_in, w_out):
    rows = lax.axis_size("row")
    total = tokens.shape[0] * rows

    def fetched(flip):
        return lax.ppermute(w_out, ("h", "k"), [(i, i ^ flip) for i in range(4)])

    chip, cross = fetched(2), fetched(3)
    beside = fetched(1)
    projected = project(tokens, w_in, norm_gain)
    arrived = lax.all_to_all(projected, "row", 0, 0, tiled=True)
    core = lax.axis_index("k").astype(jnp.int32).reshape(1)
    place = lax.axis_index(("h", "k")).astype(jnp.int32).reshape(1)
    arrived, core, place = lax.optimization_barrier((arrived, core, place))
    spectra = positions(arrived, total)
    arrived = lax.all_to_all(spectra, ("row", "h"), 0, 0, tiled=True)
    arrived = lax.all_gather(arrived.reshape(2 * rows, 2, *arrived.shape[1:]), "k", axis=0)
    mixed = channel_mix(core, arrived, channel_table(rows))
    gathered = lax.all_gather(mixed, "g", axis=0)
    output = output_map(place, gathered, w_out, beside, chip, cross)
    output = lax.all_to_all(output, ("h", "k"), 0, 0, tiled=True)
    return output.reshape(tokens.shape[0], w_out.shape[1])


def solution(mesh):
    mesh = Mesh(mesh.devices.reshape(32, 4, 2, 2), ("row", "g", "h", "k"))
    columns = ("g", "h", "k")
    placed = (P("row", None), P(), P(None, columns), P(None, columns))
    return jax.shard_map(
        local, mesh=mesh, in_specs=placed, out_specs=P("row", columns), check_vma=False
    )
```

```python
import math

import jax
import jax.numpy as jnp
import numpy as np
from jax import lax
from jax.experimental import pallas as pl
from jax.experimental.pallas import tpu as pltpu
from jax.sharding import Mesh
from jax.sharding import PartitionSpec as P


GROUP = 256
NORM_EPS = 1e-06
BLOCK = 128
AHEAD = 3
SMALL = pltpu.CompilerParams(vmem_limit_bytes=16 << 20)


def project_body(x_hbm, w_hbm, gain_hbm, out_ref, x_buf, w_buf, gain_buf, scr, sems):
    pieces = sems.shape[0] - 2
    rows = x_buf.shape[0] // pieces
    weights = pltpu.make_async_copy(w_hbm, w_buf, sems.at[pieces])
    gains = pltpu.make_async_copy(gain_hbm, gain_buf, sems.at[pieces + 1])
    weights.start()
    gains.start()
    copies = []
    for j in range(pieces):
        span = pl.ds(rows * j, rows)
        copies.append(pltpu.make_async_copy(x_hbm.at[span], x_buf.at[span], sems.at[j]))
    for j in range(AHEAD):
        copies[j].start()
    weights.wait()
    gains.wait()
    weight = (w_buf[...].astype(jnp.float32) * gain_buf[...]).T.astype(jnp.bfloat16)
    half = weight.shape[1] // 2
    blocks = x_buf.shape[0] // BLOCK


    def finish(j, part, square):
        turned = (part * lax.rsqrt(square + NORM_EPS)).T
        for b in range(rows // BLOCK):
            for c in range(2):
                place = rows // BLOCK * j + b + blocks * c
                scr[:, place, :] = turned[half * c : half * c + half, BLOCK * b : BLOCK * b + BLOCK]

    waiting = None
    for j in range(pieces):
        copies[j].wait()
        if j + AHEAD < pieces:
            copies[j + AHEAD].start()
        x = x_buf[rows * j : rows * j + rows, :]
        wide = x.astype(jnp.float32)
        square = jnp.mean(wide * wide, axis=1, keepdims=True)
        part = jnp.dot(x, weight, preferred_element_type=jnp.float32)
        if waiting is not None:
            finish(*waiting)
        waiting = (j, part, square)
    finish(*waiting)
    out_ref[...] = scr[...].astype(jnp.bfloat16)


def project(tokens, w_in, gain):
    rows, width = tokens.shape
    channels = w_in.shape[1]
    pieces = 4
    shape = (channels // 2, 2 * rows // BLOCK, BLOCK)
    inputs = [
        pltpu.with_memory_space_constraint(a, pltpu.HBM) for a in (tokens, w_in.T, gain[None])
    ]
    return pl.pallas_call(
        project_body,
        in_specs=[pl.BlockSpec(memory_space=pltpu.HBM)] * 3,
        out_specs=pl.BlockSpec(memory_space=pltpu.VMEM),
        out_shape=pltpu.VMEM(shape, jnp.bfloat16),
        scratch_shapes=[
            pltpu.VMEM((rows, width), jnp.bfloat16),
            pltpu.VMEM((channels, width), jnp.bfloat16),
            pltpu.VMEM((1, width), jnp.float32),
            pltpu.VMEM(shape, jnp.float32),
            pltpu.SemaphoreType.DMA((pieces + 2,)),
        ],
        compiler_params=pltpu.CompilerParams(vmem_limit_bytes=24 << 20),
    )(*inputs)


def fft_tables(total, n_first, n_second):
    scale = 1.0 / math.sqrt(total * GROUP)
    one = np.arange(n_first)
    two = np.arange(n_second)
    first = 2.0 * np.pi * (np.outer(one, one) % n_first) / n_first
    table_one = np.concatenate([np.cos(first), np.sin(first)], 0)
    turn = 2.0 * np.pi * np.outer(one, two) / total
    turns = np.stack([np.cos(turn), np.sin(turn)]) * scale
    second = 2.0 * np.pi * (np.outer(two, two) % n_second) / n_second
    cosine, sine = np.cos(second), np.sin(second)
    table_two = np.block([[cosine, sine], [-sine, cosine]])
    return (
        jnp.asarray(table_one, jnp.bfloat16),
        jnp.asarray(turns, jnp.float32),
        jnp.asarray(table_two, jnp.bfloat16),
    )


def positions_body(x_ref, one_ref, turn_ref, two_ref, out_ref, scr):
    wide = x_ref[...].astype(jnp.float32)
    n_first = wide.shape[0] * 8
    both = [
        wide[:, 8 * c : 8 * c + 8, :].reshape(n_first, BLOCK).astype(jnp.bfloat16)
        for c in range(2)
    ]
    cosine, sine = turn_ref[0], turn_ref[1]
    for c in range(2):
        y = jnp.dot(one_ref[...], both[c], preferred_element_type=jnp.float32)
        y_cos, y_sin = y[:n_first], y[n_first:]
        turned = jnp.concatenate(
            [y_cos * cosine - y_sin * sine, -(y_sin * cosine) - y_cos * sine], 1
        ).astype(jnp.bfloat16)
        z = lax.dot_general(
            two_ref[...], turned, (((1,), (1,)), ((), ())), preferred_element_type=jnp.float32
        )
        for part in range(2):
            for high in range(2):
                scr[:, 4 * c + 2 * part + high, :] = z[
                    BLOCK * part : BLOCK * part + BLOCK, BLOCK * high : BLOCK * high + BLOCK
                ]
    out_ref[...] = scr[...].astype(jnp.bfloat16)


def positions(arrived, total):
    rows = arrived.shape[0]
    tables = fft_tables(total, rows * 8, BLOCK)
    shape = (BLOCK, 8, BLOCK)
    return pl.pallas_call(
        positions_body,
        out_shape=pltpu.VMEM(shape, jnp.bfloat16),
        scratch_shapes=[pltpu.VMEM(shape, jnp.float32)],
        compiler_params=SMALL,
    )(arrived, *tables)


def channel_table(rows):
    source = np.arange(4 * rows)
    core, row, half = source // (2 * rows), source // 2 % rows, source % 2
    place = 2 * half + core
    channel = np.stack([GROUP // 4 * place + row + rows * c for c in range(2)])
    freq = np.arange(GROUP)
    phase = 2.0 * np.pi * (freq[:, None, None] * channel[None] % GROUP) / GROUP
    both = np.stack([np.cos(phase), np.sin(phase)], 2)
    return jnp.asarray(both.reshape(GROUP, -1), jnp.bfloat16)


def channels_body(core_ref, x_ref, table_ref, out_ref, scr):
    core = core_ref[0]
    for k in range(2):
        part = x_ref[k, :, pl.ds(core, 1)]
        count = part.shape[0]
        scr[count * k : count * k + count] = part.reshape(count, *scr.shape[1:]).astype(jnp.float32)
    rows = [
        jnp.concatenate([scr[:, 2 * j, :], scr[:, 2 * j + 1, :]], 1).astype(jnp.bfloat16)
        for j in range(4)
    ]
    data = jnp.concatenate(rows, 0)
    spectrum = jnp.dot(table_ref[...], data, preferred_element_type=jnp.float32)
    out_ref[...] = spectrum.T.astype(jnp.bfloat16)


def channel_mix(core, arrived, table):
    sources, height, width = arrived.shape[1], *arrived.shape[3:]
    return pl.pallas_call(
        channels_body,
        in_specs=[
            pl.BlockSpec(memory_space=pltpu.SMEM),
            pl.BlockSpec(memory_space=pltpu.VMEM),
            pl.BlockSpec(memory_space=pltpu.VMEM),
        ],
        out_shape=pltpu.VMEM((height * width // 4, GROUP), jnp.bfloat16),
        scratch_shapes=[pltpu.VMEM((2 * sources, height, width), jnp.float32)],
        compiler_params=SMALL,
    )(core, arrived, table)


def output_body(spec_ref, *refs):
    weights, outs = refs[: len(refs) // 2], refs[len(refs) // 2 :]
    groups = spec_ref.shape[0]
    for ref, out_ref in zip(weights, outs):
        total = None
        for g in range(groups):
            part = jnp.dot(
                spec_ref[g],
                ref[GROUP * g : GROUP * g + GROUP, :],
                preferred_element_type=jnp.float32,
            )
            total = part if total is None else total + part
        out_ref[...] = total.astype(jnp.bfloat16)


def output_map(gathered, *weights):
    part = pltpu.VMEM((gathered.shape[1], weights[0].shape[1]), jnp.bfloat16)
    return pl.pallas_call(
        output_body, out_shape=[part] * len(weights), compiler_params=SMALL
    )(gathered, *weights)


def join_body(place_ref, *refs):
    *parts, out_ref, sems = refs
    count = parts[0].shape[0]
    copies = []
    for flip, part in enumerate(parts):
        span = pl.ds(pl.multiple_of((place_ref[0] ^ flip) * count, count), count)
        copies.append(pltpu.make_async_copy(part, out_ref.at[span], sems.at[flip]))
        copies[flip].start()
    for copy in copies:
        copy.wait()


def join(place, *parts):
    count, width = parts[0].shape
    whole = pl.BlockSpec(memory_space=pltpu.VMEM)
    return pl.pallas_call(
        join_body,
        in_specs=[pl.BlockSpec(memory_space=pltpu.SMEM)] + [whole] * len(parts),
        out_specs=pl.BlockSpec(memory_space=pltpu.HBM),
        out_shape=jax.ShapeDtypeStruct((count * len(parts), width), jnp.bfloat16),
        scratch_shapes=[pltpu.SemaphoreType.DMA((len(parts),))],
        compiler_params=SMALL,
    )(place, *parts)


def local(tokens, norm_gain, w_in, w_out):
    rows = lax.axis_size("row")
    total = tokens.shape[0] * rows

    def sent(part, flip):
        return lax.ppermute(part, ("h", "k"), [(i, i ^ flip) for i in range(4)])

    w_chip, w_cross = sent(w_out, 2), sent(w_out, 3)
    w_core = sent(w_out, 1)
    projected = project(tokens, w_in, norm_gain)
    arrived = lax.all_to_all(projected, "row", 0, 0, tiled=True)
    spectra = positions(arrived, total)
    arrived = lax.all_to_all(spectra, ("row", "h"), 0, 0, tiled=True)
    arrived = lax.all_gather(arrived.reshape(2 * rows, 2, *arrived.shape[1:]), "k", axis=0)
    core = lax.axis_index("k").astype(jnp.int32).reshape(1)
    mixed = channel_mix(core, arrived, channel_table(rows))
    gathered = lax.all_gather(mixed, "g", axis=0)
    chip, cross = output_map(gathered, w_chip, w_cross)
    chip, cross = sent(chip, 2), sent(cross, 3)
    mine, near = output_map(gathered, w_out, w_core)
    near = sent(near, 1)
    place = lax.axis_index(("h", "k")).astype(jnp.int32).reshape(1)
    return join(place, mine, near, chip, cross)


def solution(mesh):
    mesh = Mesh(mesh.devices.reshape(32, 4, 2, 2), ("row", "g", "h", "k"))
    columns = ("g", "h", "k")
    placed = (P("row", None), P(), P(None, columns), P(None, columns))
    return jax.shard_map(
        local, mesh=mesh, in_specs=placed, out_specs=P("row", columns), check_vma=False
    )
```

```python
import math

import jax
import jax.numpy as jnp
import numpy as np
from jax import lax
from jax.experimental import pallas as pl
from jax.experimental.pallas import tpu as pltpu
from jax.sharding import Mesh
from jax.sharding import PartitionSpec as P


GROUP = 256
NORM_EPS = 1e-06
BLOCK = 128
AHEAD = 3
SMALL = pltpu.CompilerParams(vmem_limit_bytes=16 << 20)


def project_body(x_hbm, w_hbm, gain_hbm, out_ref, x_buf, w_buf, gain_buf, scr, sems):
    pieces = sems.shape[0] - 2
    rows = x_buf.shape[0] // pieces
    weights = pltpu.make_async_copy(w_hbm, w_buf, sems.at[pieces])
    gains = pltpu.make_async_copy(gain_hbm, gain_buf, sems.at[pieces + 1])
    weights.start()
    gains.start()
    copies = []
    for j in range(pieces):
        span = pl.ds(rows * j, rows)
        copies.append(pltpu.make_async_copy(x_hbm.at[span], x_buf.at[span], sems.at[j]))
    for j in range(AHEAD):
        copies[j].start()
    weights.wait()
    gains.wait()
    weight = (w_buf[...].astype(jnp.float32) * gain_buf[...]).T.astype(jnp.bfloat16)
    half = weight.shape[1] // 2
    blocks = x_buf.shape[0] // BLOCK


    def finish(j, part, square):
        turned = (part * lax.rsqrt(square + NORM_EPS)).T
        for b in range(rows // BLOCK):
            for c in range(2):
                place = rows // BLOCK * j + b + blocks * c
                scr[:, place, :] = turned[half * c : half * c + half, BLOCK * b : BLOCK * b + BLOCK]

    waiting = None
    for j in range(pieces):
        copies[j].wait()
        if j + AHEAD < pieces:
            copies[j + AHEAD].start()
        x = x_buf[rows * j : rows * j + rows, :]
        wide = x.astype(jnp.float32)
        square = jnp.mean(wide * wide, axis=1, keepdims=True)
        part = jnp.dot(x, weight, preferred_element_type=jnp.float32)
        if waiting is not None:
            finish(*waiting)
        waiting = (j, part, square)
    finish(*waiting)
    out_ref[...] = scr[...].astype(jnp.bfloat16)


def project(tokens, w_in, gain):
    rows, width = tokens.shape
    channels = w_in.shape[1]
    pieces = 4
    shape = (channels // 2, 2 * rows // BLOCK, BLOCK)
    inputs = [
        pltpu.with_memory_space_constraint(a, pltpu.HBM) for a in (tokens, w_in.T, gain[None])
    ]
    return pl.pallas_call(
        project_body,
        in_specs=[pl.BlockSpec(memory_space=pltpu.HBM)] * 3,
        out_specs=pl.BlockSpec(memory_space=pltpu.VMEM),
        out_shape=pltpu.VMEM(shape, jnp.bfloat16),
        scratch_shapes=[
            pltpu.VMEM((rows, width), jnp.bfloat16),
            pltpu.VMEM((channels, width), jnp.bfloat16),
            pltpu.VMEM((1, width), jnp.float32),
            pltpu.VMEM(shape, jnp.float32),
            pltpu.SemaphoreType.DMA((pieces + 2,)),
        ],
        compiler_params=pltpu.CompilerParams(vmem_limit_bytes=24 << 20),
    )(*inputs)


def fft_tables(total, n_first, n_second):
    scale = 1.0 / math.sqrt(total * GROUP)
    one = np.arange(n_first)
    two = np.arange(n_second)
    first = 2.0 * np.pi * (np.outer(one, one) % n_first) / n_first
    table_one = np.concatenate([np.cos(first), np.sin(first)], 0)
    turn = 2.0 * np.pi * np.outer(one, two) / total
    turns = np.stack([np.cos(turn), np.sin(turn)]) * scale
    second = 2.0 * np.pi * (np.outer(two, two) % n_second) / n_second
    cosine, sine = np.cos(second), np.sin(second)
    table_two = np.block([[cosine, sine], [-sine, cosine]])
    return (
        jnp.asarray(table_one, jnp.bfloat16),
        jnp.asarray(turns, jnp.float32),
        jnp.asarray(table_two, jnp.bfloat16),
    )


def positions_body(x_ref, one_ref, turn_ref, two_ref, out_ref, scr):
    wide = x_ref[...].astype(jnp.float32)
    n_first = wide.shape[0] * 8
    both = [
        wide[:, 8 * c : 8 * c + 8, :].reshape(n_first, BLOCK).astype(jnp.bfloat16)
        for c in range(2)
    ]
    cosine, sine = turn_ref[0], turn_ref[1]
    for c in range(2):
        y = jnp.dot(one_ref[...], both[c], preferred_element_type=jnp.float32)
        y_cos, y_sin = y[:n_first], y[n_first:]
        turned = jnp.concatenate(
            [y_cos * cosine - y_sin * sine, -(y_sin * cosine) - y_cos * sine], 1
        ).astype(jnp.bfloat16)
        z = lax.dot_general(
            two_ref[...], turned, (((1,), (1,)), ((), ())), preferred_element_type=jnp.float32
        )
        for part in range(2):
            for high in range(2):
                scr[:, 4 * c + 2 * part + high, :] = z[
                    BLOCK * part : BLOCK * part + BLOCK, BLOCK * high : BLOCK * high + BLOCK
                ]
    out_ref[...] = scr[...].astype(jnp.bfloat16)


def positions(arrived, total):
    rows = arrived.shape[0]
    tables = fft_tables(total, rows * 8, BLOCK)
    shape = (BLOCK, 8, BLOCK)
    return pl.pallas_call(
        positions_body,
        out_shape=pltpu.VMEM(shape, jnp.bfloat16),
        scratch_shapes=[pltpu.VMEM(shape, jnp.float32)],
        compiler_params=SMALL,
    )(arrived, *tables)


def channel_table(rows):
    source = np.arange(4 * rows)
    core, row, half = source // (2 * rows), source // 2 % rows, source % 2
    place = 2 * half + core
    channel = np.stack([GROUP // 4 * place + row + rows * c for c in range(2)])
    freq = np.arange(GROUP)
    phase = 2.0 * np.pi * (freq[:, None, None] * channel[None] % GROUP) / GROUP
    both = np.stack([np.cos(phase), np.sin(phase)], 2)
    return jnp.asarray(both.reshape(GROUP, -1), jnp.bfloat16)


def channels_body(core_ref, x_ref, table_ref, out_ref, scr):
    core = core_ref[0]
    for k in range(2):
        part = x_ref[k, :, pl.ds(core, 1)]
        count = part.shape[0]
        scr[count * k : count * k + count] = part.reshape(count, *scr.shape[1:]).astype(jnp.float32)
    rows = [
        jnp.concatenate([scr[:, 2 * j, :], scr[:, 2 * j + 1, :]], 1).astype(jnp.bfloat16)
        for j in range(4)
    ]
    data = jnp.concatenate(rows, 0)
    spectrum = jnp.dot(table_ref[...], data, preferred_element_type=jnp.float32)
    out_ref[...] = spectrum.T.astype(jnp.bfloat16)


def channel_mix(core, arrived, table):
    sources, height, width = arrived.shape[1], *arrived.shape[3:]
    return pl.pallas_call(
        channels_body,
        in_specs=[
            pl.BlockSpec(memory_space=pltpu.SMEM),
            pl.BlockSpec(memory_space=pltpu.VMEM),
            pl.BlockSpec(memory_space=pltpu.VMEM),
        ],
        out_shape=pltpu.VMEM((height * width // 4, GROUP), jnp.bfloat16),
        scratch_shapes=[pltpu.VMEM((2 * sources, height, width), jnp.float32)],
        compiler_params=SMALL,
    )(core, arrived, table)


def output_body(chip_ref, spec_ref, *refs):
    *weights, out_ref = refs
    groups = spec_ref.shape[0]
    for flip, ref in enumerate(weights):
        total = None
        for g in range(groups):
            part = jnp.dot(
                spec_ref[g],
                ref[GROUP * g : GROUP * g + GROUP, :],
                preferred_element_type=jnp.float32,
            )
            total = part if total is None else total + part
        out_ref[pl.ds(chip_ref[0] ^ flip, 1)] = total.astype(jnp.bfloat16)[None]


def output_map(chip, gathered, *weights):
    count = gathered.shape[1]
    whole = pl.BlockSpec(memory_space=pltpu.VMEM)
    return pl.pallas_call(
        output_body,
        in_specs=[pl.BlockSpec(memory_space=pltpu.SMEM)] + [whole] * (1 + len(weights)),
        out_shape=pltpu.VMEM((len(weights), count, weights[0].shape[1]), jnp.bfloat16),
        compiler_params=SMALL,
    )(chip, gathered, *weights)


def local(tokens, norm_gain, w_in, w_out):
    rows = lax.axis_size("row")
    total = tokens.shape[0] * rows

    def sent(part, flip):
        return lax.ppermute(part, ("h", "k"), [(i, i ^ flip) for i in range(4)])

    chip = sent(w_out, 2)
    beside = sent(w_out, 1)
    cross = sent(beside, 2)
    projected = project(tokens, w_in, norm_gain)
    arrived = lax.all_to_all(projected, "row", 0, 0, tiled=True)
    spectra = positions(arrived, total)
    arrived = lax.all_to_all(spectra, ("row", "h"), 0, 0, tiled=True)
    arrived = lax.all_gather(arrived.reshape(2 * rows, 2, *arrived.shape[1:]), "k", axis=0)
    core = lax.axis_index("k").astype(jnp.int32).reshape(1)
    mixed = channel_mix(core, arrived, channel_table(rows))
    gathered = lax.all_gather(mixed, "g", axis=0)
    place = lax.axis_index(("h", "k")).astype(jnp.int32).reshape(1)
    output = output_map(place, gathered, w_out, beside, chip, cross)
    output = lax.all_to_all(output, ("h", "k"), 0, 0, tiled=True)
    return output.reshape(tokens.shape[0], w_out.shape[1])


def solution(mesh):
    mesh = Mesh(mesh.devices.reshape(32, 4, 2, 2), ("row", "g", "h", "k"))
    columns = ("g", "h", "k")
    placed = (P("row", None), P(), P(None, columns), P(None, columns))
    return jax.shard_map(
        local, mesh=mesh, in_specs=placed, out_specs=P("row", columns), check_vma=False
    )
```

```python
import math

import jax
import jax.numpy as jnp
import numpy as np
from jax import lax
from jax.experimental import pallas as pl
from jax.experimental.pallas import tpu as pltpu
from jax.sharding import Mesh
from jax.sharding import PartitionSpec as P

GROUP = 256
NORM_EPS = 1e-06
BLOCK = 128
AHEAD = 3
SMALL = pltpu.CompilerParams(vmem_limit_bytes=16 << 20)


def project_body(x_hbm, w_hbm, gain_hbm, out_ref, x_buf, w_buf, gain_buf, scr, sems):
    pieces = sems.shape[0] - 2
    rows = x_buf.shape[0] // pieces
    weights = pltpu.make_async_copy(w_hbm, w_buf, sems.at[pieces])
    gains = pltpu.make_async_copy(gain_hbm, gain_buf, sems.at[pieces + 1])
    weights.start()
    gains.start()
    copies = []
    for j in range(pieces):
        span = pl.ds(rows * j, rows)
        copies.append(pltpu.make_async_copy(x_hbm.at[span], x_buf.at[span], sems.at[j]))
    for j in range(AHEAD):
        copies[j].start()
    weights.wait()
    gains.wait()
    weight = (w_buf[...].astype(jnp.float32) * gain_buf[...]).T.astype(jnp.bfloat16)
    half = weight.shape[1] // 2
    blocks = x_buf.shape[0] // BLOCK


    def finish(j, part, square):
        turned = (part * lax.rsqrt(square + NORM_EPS)).T
        for b in range(rows // BLOCK):
            for c in range(2):
                place = rows // BLOCK * j + b + blocks * c
                scr[:, place, :] = turned[half * c : half * c + half, BLOCK * b : BLOCK * b + BLOCK]

    waiting = None
    for j in range(pieces):
        copies[j].wait()
        if j + AHEAD < pieces:
            copies[j + AHEAD].start()
        x = x_buf[rows * j : rows * j + rows, :]
        wide = x.astype(jnp.float32)
        square = jnp.mean(wide * wide, axis=1, keepdims=True)
        part = jnp.dot(x, weight, preferred_element_type=jnp.float32)
        if waiting is not None:
            finish(*waiting)
        waiting = (j, part, square)
    finish(*waiting)
    out_ref[...] = scr[...].astype(jnp.bfloat16)


def project(tokens, w_in, gain):
    rows, width = tokens.shape
    channels = w_in.shape[1]
    pieces = 4
    shape = (channels // 2, 2 * rows // BLOCK, BLOCK)
    inputs = [
        pltpu.with_memory_space_constraint(a, pltpu.HBM) for a in (tokens, w_in.T, gain[None])
    ]
    return pl.pallas_call(
        project_body,
        in_specs=[pl.BlockSpec(memory_space=pltpu.HBM)] * 3,
        out_specs=pl.BlockSpec(memory_space=pltpu.VMEM),
        out_shape=pltpu.VMEM(shape, jnp.bfloat16),
        scratch_shapes=[
            pltpu.VMEM((rows, width), jnp.bfloat16),
            pltpu.VMEM((channels, width), jnp.bfloat16),
            pltpu.VMEM((1, width), jnp.float32),
            pltpu.VMEM(shape, jnp.float32),
            pltpu.SemaphoreType.DMA((pieces + 2,)),
        ],
        compiler_params=pltpu.CompilerParams(vmem_limit_bytes=24 << 20),
    )(*inputs)


def fft_tables(total, n_first, n_second):
    scale = 1.0 / math.sqrt(total * GROUP)
    one = np.arange(n_first)
    two = np.arange(n_second)
    first = 2.0 * np.pi * (np.outer(one, one) % n_first) / n_first
    table_one = np.concatenate([np.cos(first), np.sin(first)], 0)
    turn = 2.0 * np.pi * np.outer(one, two) / total
    turns = np.stack([np.cos(turn), np.sin(turn)]) * scale
    second = 2.0 * np.pi * (np.outer(two, two) % n_second) / n_second
    cosine, sine = np.cos(second), np.sin(second)
    table_two = np.block([[cosine, sine], [-sine, cosine]])
    return (
        jnp.asarray(table_one, jnp.bfloat16),
        jnp.asarray(turns, jnp.float32),
        jnp.asarray(table_two, jnp.bfloat16),
    )


def positions_body(x_ref, one_ref, turn_ref, two_ref, out_ref, scr):
    wide = x_ref[...].astype(jnp.float32)
    n_first = wide.shape[0] * 8
    both = [
        wide[:, 8 * c : 8 * c + 8, :].reshape(n_first, BLOCK).astype(jnp.bfloat16)
        for c in range(2)
    ]
    cosine, sine = turn_ref[0], turn_ref[1]
    for c in range(2):
        y = jnp.dot(one_ref[...], both[c], preferred_element_type=jnp.float32)
        y_cos, y_sin = y[:n_first], y[n_first:]
        turned = jnp.concatenate(
            [y_cos * cosine - y_sin * sine, -(y_sin * cosine) - y_cos * sine], 1
        ).astype(jnp.bfloat16)
        z = lax.dot_general(
            two_ref[...], turned, (((1,), (1,)), ((), ())), preferred_element_type=jnp.float32
        )
        for part in range(2):
            for high in range(2):
                scr[:, 4 * c + 2 * part + high, :] = z[
                    BLOCK * part : BLOCK * part + BLOCK, BLOCK * high : BLOCK * high + BLOCK
                ]
    out_ref[...] = scr[...].astype(jnp.bfloat16)


def positions(arrived, total):
    rows = arrived.shape[0]
    tables = fft_tables(total, rows * 8, BLOCK)
    shape = (BLOCK, 8, BLOCK)
    return pl.pallas_call(
        positions_body,
        out_shape=pltpu.VMEM(shape, jnp.bfloat16),
        scratch_shapes=[pltpu.VMEM(shape, jnp.float32)],
        compiler_params=SMALL,
    )(arrived, *tables)


def channel_table(rows):
    source = np.arange(4 * rows)
    core, row, half = source // (2 * rows), source // 2 % rows, source % 2
    place = 2 * half + core
    channel = np.stack([GROUP // 4 * place + row + rows * c for c in range(2)])
    freq = np.arange(GROUP)
    phase = 2.0 * np.pi * (freq[:, None, None] * channel[None] % GROUP) / GROUP
    both = np.stack([np.cos(phase), np.sin(phase)], 2)
    return jnp.asarray(both.reshape(GROUP, -1), jnp.bfloat16)


def channels_body(core_ref, x_ref, table_ref, out_ref, scr):
    core = core_ref[0]
    for k in range(2):
        part = x_ref[k, :, pl.ds(core, 1)]
        count = part.shape[0]
        scr[count * k : count * k + count] = part.reshape(count, *scr.shape[1:]).astype(jnp.float32)
    rows = [
        jnp.concatenate([scr[:, 2 * j, :], scr[:, 2 * j + 1, :]], 1).astype(jnp.bfloat16)
        for j in range(4)
    ]
    data = jnp.concatenate(rows, 0)
    spectrum = jnp.dot(table_ref[...], data, preferred_element_type=jnp.float32)
    out_ref[...] = spectrum.T.astype(jnp.bfloat16)


def channel_mix(core, arrived, table):
    sources, height, width = arrived.shape[1], *arrived.shape[3:]
    return pl.pallas_call(
        channels_body,
        in_specs=[
            pl.BlockSpec(memory_space=pltpu.SMEM),
            pl.BlockSpec(memory_space=pltpu.VMEM),
            pl.BlockSpec(memory_space=pltpu.VMEM),
        ],
        out_shape=pltpu.VMEM((height * width // 4, GROUP), jnp.bfloat16),
        scratch_shapes=[pltpu.VMEM((2 * sources, height, width), jnp.float32)],
        compiler_params=SMALL,
    )(core, arrived, table)


def output_body(half_ref, spec_ref, own_ref, other_ref, out_ref):
    half = half_ref[0]
    spectra = jnp.concatenate([spec_ref[g] for g in range(spec_ref.shape[0])], 1)
    for ref, place in ((own_ref, 2 * half), (other_ref, 2 * (1 - half))):
        weights = jnp.concatenate([ref[0], ref[1]], 1)
        total = jnp.dot(spectra, weights, preferred_element_type=jnp.float32)
        total = total.astype(jnp.bfloat16)
        width = total.shape[1] // 2
        for k in range(2):
            out_ref[pl.ds(place + k, 1)] = total[:, width * k : width * k + width][None]


def output_map(half, gathered, own, other):
    count = gathered.shape[1]
    return pl.pallas_call(
        output_body,
        in_specs=[
            pl.BlockSpec(memory_space=pltpu.SMEM),
            pl.BlockSpec(memory_space=pltpu.VMEM),
            pl.BlockSpec(memory_space=pltpu.VMEM),
            pl.BlockSpec(memory_space=pltpu.VMEM),
        ],
        out_shape=pltpu.VMEM((4, count, own.shape[2]), jnp.bfloat16),
        compiler_params=SMALL,
    )(half, gathered, own, other)


def local(tokens, norm_gain, w_in, w_out):
    rows = lax.axis_size("row")
    total = tokens.shape[0] * rows
    own = lax.all_gather(w_out, "k", axis=0)
    other = lax.ppermute(own, "h", [(0, 1), (1, 0)])
    projected = project(tokens, w_in, norm_gain)
    arrived = lax.all_to_all(projected, "row", 0, 0, tiled=True)
    spectra = positions(arrived, total)
    arrived = lax.all_to_all(spectra, ("row", "h"), 0, 0, tiled=True)
    arrived = lax.all_gather(arrived.reshape(2 * rows, 2, *arrived.shape[1:]), "k", axis=0)
    core = lax.axis_index("k").astype(jnp.int32).reshape(1)
    mixed = channel_mix(core, arrived, channel_table(rows))
    gathered = lax.all_gather(mixed, "g", axis=0)
    half = lax.axis_index("h").astype(jnp.int32).reshape(1)
    output = output_map(half, gathered, own, other)
    output = lax.all_to_all(output, ("h", "k"), 0, 0, tiled=True)
    return output.reshape(tokens.shape[0], w_out.shape[1])


def solution(mesh):
    mesh = Mesh(mesh.devices.reshape(32, 4, 2, 2), ("row", "g", "h", "k"))
    columns = ("g", "h", "k")
    placed = (P("row", None), P(), P(None, columns), P(None, columns))
    return jax.shard_map(
        local, mesh=mesh, in_specs=placed, out_specs=P("row", columns), check_vma=False
    )
```

```python
import math

import jax
import jax.numpy as jnp
import numpy as np
from jax import lax
from jax.experimental import pallas as pl
from jax.experimental.pallas import tpu as pltpu
from jax.sharding import Mesh
from jax.sharding import PartitionSpec as P

GROUP = 256
NORM_EPS = 1e-06
BLOCK = 128
AHEAD = 3
SMALL = pltpu.CompilerParams(vmem_limit_bytes=16 << 20)


def project_body(x_hbm, w_hbm, gain_hbm, out_ref, x_buf, w_buf, gain_buf, scr, sems):
    pieces = sems.shape[0] - 2
    rows = x_buf.shape[0] // pieces
    weights = pltpu.make_async_copy(w_hbm, w_buf, sems.at[pieces])
    gains = pltpu.make_async_copy(gain_hbm, gain_buf, sems.at[pieces + 1])
    weights.start()
    gains.start()
    copies = []
    for j in range(pieces):
        span = pl.ds(rows * j, rows)
        copies.append(pltpu.make_async_copy(x_hbm.at[span], x_buf.at[span], sems.at[j]))
    for j in range(AHEAD):
        copies[j].start()
    weights.wait()
    gains.wait()
    weight = (w_buf[...].astype(jnp.float32) * gain_buf[...]).T.astype(jnp.bfloat16)
    half = weight.shape[1] // 2
    blocks = x_buf.shape[0] // BLOCK


    def finish(j, part, square):
        turned = (part * lax.rsqrt(square + NORM_EPS)).T
        for b in range(rows // BLOCK):
            for c in range(2):
                place = rows // BLOCK * j + b + blocks * c
                scr[:, place, :] = turned[half * c : half * c + half, BLOCK * b : BLOCK * b + BLOCK]

    waiting = None
    for j in range(pieces):
        copies[j].wait()
        if j + AHEAD < pieces:
            copies[j + AHEAD].start()
        x = x_buf[rows * j : rows * j + rows, :]
        wide = x.astype(jnp.float32)
        square = jnp.mean(wide * wide, axis=1, keepdims=True)
        part = jnp.dot(x, weight, preferred_element_type=jnp.float32)
        if waiting is not None:
            finish(*waiting)
        waiting = (j, part, square)
    finish(*waiting)
    out_ref[...] = scr[...].astype(jnp.bfloat16)


def project(tokens, w_in, gain):
    rows, width = tokens.shape
    channels = w_in.shape[1]
    pieces = 4
    shape = (channels // 2, 2 * rows // BLOCK, BLOCK)
    inputs = [
        pltpu.with_memory_space_constraint(a, pltpu.HBM) for a in (tokens, w_in.T, gain[None])
    ]
    return pl.pallas_call(
        project_body,
        in_specs=[pl.BlockSpec(memory_space=pltpu.HBM)] * 3,
        out_specs=pl.BlockSpec(memory_space=pltpu.VMEM),
        out_shape=pltpu.VMEM(shape, jnp.bfloat16),
        scratch_shapes=[
            pltpu.VMEM((rows, width), jnp.bfloat16),
            pltpu.VMEM((channels, width), jnp.bfloat16),
            pltpu.VMEM((1, width), jnp.float32),
            pltpu.VMEM(shape, jnp.float32),
            pltpu.SemaphoreType.DMA((pieces + 2,)),
        ],
        compiler_params=pltpu.CompilerParams(vmem_limit_bytes=24 << 20),
    )(*inputs)


def fft_tables(total, n_first, n_second):
    scale = 1.0 / math.sqrt(total * GROUP)
    one = np.arange(n_first)
    two = np.arange(n_second)
    first = 2.0 * np.pi * (np.outer(one, one) % n_first) / n_first
    table_one = np.concatenate([np.cos(first), np.sin(first)], 0)
    turn = 2.0 * np.pi * np.outer(one, two) / total
    turns = np.stack([np.cos(turn), np.sin(turn)]) * scale
    second = 2.0 * np.pi * (np.outer(two, two) % n_second) / n_second
    cosine, sine = np.cos(second), np.sin(second)
    table_two = np.block([[cosine, sine], [-sine, cosine]])
    return (
        jnp.asarray(table_one, jnp.bfloat16),
        jnp.asarray(turns, jnp.float32),
        jnp.asarray(table_two, jnp.bfloat16),
    )


def positions_body(x_ref, one_ref, turn_ref, two_ref, out_ref, scr):
    wide = x_ref[...].astype(jnp.float32)
    n_first = wide.shape[0] * 8
    both = [wide[:, 8 * c : 8 * c + 8, :].reshape(n_first, BLOCK) for c in range(2)]
    data = jnp.concatenate(both, 1).astype(jnp.bfloat16)
    cosine, sine = turn_ref[0], turn_ref[1]
    y = jnp.dot(one_ref[...], data, preferred_element_type=jnp.float32)
    turned = []
    for c in range(2):
        y_cos = y[:n_first, BLOCK * c : BLOCK * c + BLOCK]
        y_sin = y[n_first:, BLOCK * c : BLOCK * c + BLOCK]
        pair = [y_cos * cosine - y_sin * sine, -(y_sin * cosine) - y_cos * sine]
        turned.append(jnp.concatenate(pair, 1).astype(jnp.bfloat16))
    z = lax.dot_general(
        two_ref[...],
        jnp.concatenate(turned, 0),
        (((1,), (1,)), ((), ())),
        preferred_element_type=jnp.float32,
    )
    for c in range(2):
        for part in range(2):
            for high in range(2):
                column = n_first * c + BLOCK * high
                scr[:, 4 * c + 2 * part + high, :] = z[
                    BLOCK * part : BLOCK * part + BLOCK, column : column + BLOCK
                ]
    out_ref[...] = scr[...].astype(jnp.bfloat16)


def positions(arrived, total):
    rows = arrived.shape[0]
    tables = fft_tables(total, rows * 8, BLOCK)
    shape = (BLOCK, 8, BLOCK)
    return pl.pallas_call(
        positions_body,
        out_shape=pltpu.VMEM(shape, jnp.bfloat16),
        scratch_shapes=[pltpu.VMEM(shape, jnp.float32)],
        compiler_params=SMALL,
    )(arrived, *tables)


def channel_table(rows):
    source = np.arange(4 * rows)
    core, row, half = source // (2 * rows), source // 2 % rows, source % 2
    place = 2 * half + core
    channel = np.stack([GROUP // 4 * place + row + rows * c for c in range(2)])
    freq = np.arange(GROUP)
    phase = 2.0 * np.pi * (freq[:, None, None] * channel[None] % GROUP) / GROUP
    both = np.stack([np.cos(phase), np.sin(phase)], 2)
    return jnp.asarray(both.reshape(GROUP, -1), jnp.bfloat16)


def channels_body(core_ref, x_ref, table_ref, out_ref, scr):
    core = core_ref[0]
    for k in range(2):
        part = x_ref[k, :, pl.ds(core, 1)]
        count = part.shape[0]
        scr[count * k : count * k + count] = part.reshape(count, *scr.shape[1:]).astype(jnp.float32)
    rows = [
        jnp.concatenate([scr[:, 2 * j, :], scr[:, 2 * j + 1, :]], 1).astype(jnp.bfloat16)
        for j in range(4)
    ]
    data = jnp.concatenate(rows, 0)
    spectrum = jnp.dot(table_ref[...], data, preferred_element_type=jnp.float32)
    out_ref[...] = spectrum.T.astype(jnp.bfloat16)


def channel_mix(core, arrived, table):
    sources, height, width = arrived.shape[1], *arrived.shape[3:]
    return pl.pallas_call(
        channels_body,
        in_specs=[
            pl.BlockSpec(memory_space=pltpu.SMEM),
            pl.BlockSpec(memory_space=pltpu.VMEM),
            pl.BlockSpec(memory_space=pltpu.VMEM),
        ],
        out_shape=pltpu.VMEM((height * width // 4, GROUP), jnp.bfloat16),
        scratch_shapes=[pltpu.VMEM((2 * sources, height, width), jnp.float32)],
        compiler_params=SMALL,
    )(core, arrived, table)


def output_body(half_ref, spec_ref, own_ref, other_ref, out_ref):
    half = half_ref[0]
    spectra = jnp.concatenate([spec_ref[g] for g in range(spec_ref.shape[0])], 1)
    for ref, place in ((own_ref, 2 * half), (other_ref, 2 * (1 - half))):
        weights = jnp.concatenate([ref[0], ref[1]], 1)
        total = jnp.dot(spectra, weights, preferred_element_type=jnp.float32)
        total = total.astype(jnp.bfloat16)
        width = total.shape[1] // 2
        for k in range(2):
            out_ref[pl.ds(place + k, 1)] = total[:, width * k : width * k + width][None]


def output_map(half, gathered, own, other):
    count = gathered.shape[1]
    return pl.pallas_call(
        output_body,
        in_specs=[
            pl.BlockSpec(memory_space=pltpu.SMEM),
            pl.BlockSpec(memory_space=pltpu.VMEM),
            pl.BlockSpec(memory_space=pltpu.VMEM),
            pl.BlockSpec(memory_space=pltpu.VMEM),
        ],
        out_shape=pltpu.VMEM((4, count, own.shape[2]), jnp.bfloat16),
        compiler_params=SMALL,
    )(half, gathered, own, other)


def local(tokens, norm_gain, w_in, w_out):
    rows = lax.axis_size("row")
    total = tokens.shape[0] * rows
    own = lax.all_gather(w_out, "k", axis=0)
    other = lax.ppermute(own, "h", [(0, 1), (1, 0)])
    projected = project(tokens, w_in, norm_gain)
    arrived = lax.all_to_all(projected, "row", 0, 0, tiled=True)
    spectra = positions(arrived, total)
    arrived = lax.all_to_all(spectra, ("row", "h"), 0, 0, tiled=True)
    arrived = lax.all_gather(arrived.reshape(2 * rows, 2, *arrived.shape[1:]), "k", axis=0)
    core = lax.axis_index("k").astype(jnp.int32).reshape(1)
    mixed = channel_mix(core, arrived, channel_table(rows))
    gathered = lax.all_gather(mixed, "g", axis=0)
    half = lax.axis_index("h").astype(jnp.int32).reshape(1)
    output = output_map(half, gathered, own, other)
    output = lax.all_to_all(output, ("h", "k"), 0, 0, tiled=True)
    return output.reshape(tokens.shape[0], w_out.shape[1])


def solution(mesh):
    mesh = Mesh(mesh.devices.reshape(32, 4, 2, 2), ("row", "g", "h", "k"))
    columns = ("g", "h", "k")
    placed = (P("row", None), P(), P(None, columns), P(None, columns))
    return jax.shard_map(
        local, mesh=mesh, in_specs=placed, out_specs=P("row", columns), check_vma=False
    )
```
